256 devices in a mesh: sp: 128 (over z, y, x), tp: 2 (over core).
Axes of the slice: x: 4, y: 4, z: 8, core: 2. Of those that a mesh axis runs over, the one named last changes fastest.
Arguments:
- hidden: bfloat16 [32768, 2048], P('sp', 'tp'), may hold values from -16 to 16
- query_weight: bfloat16 [2048, 1024], P(None, 'tp'), may hold values from -0.125 to 0.125
- key_weight: bfloat16 [2048, 512], P(None, 'tp'), may hold values from -0.125 to 0.125
- value_weight: bfloat16 [2048, 512], P(None, 'tp'), may hold values from -0.125 to 0.125
- head_gate_weight: bfloat16 [2048, 1024], P(None, 'tp'), may hold values from -0.125 to 0.125
- state_in_weight: bfloat16 [2048, 1024], P(None, 'tp'), may hold values from -0.125 to 0.125
- state_gate_weight: bfloat16 [2048, 1024], P(None, 'tp'), may hold values from -0.125 to 0.125
- sink_logit: float32 [16], P('tp'), may hold values from 1 to 6
- decay_real: float32 [64, 64], P('tp'), may hold values from -0.7 to -0.0049
- decay_frequency: float32 [64, 64], P('tp'), may hold values from 0 to 192
- log_step: float32 [64], P('tp'), may hold values from -20 to 0
- input_real: float32 [64, 64, 16], P('tp'), may hold values from -8196 to 8196
- input_imaginary: float32 [64, 64, 16], P('tp'), may hold values from -8196 to 8196
- output_real: float32 [64, 16, 64], P('tp'), may hold values from -0.5 to 0.5
- output_imaginary: float32 [64, 16, 64], P('tp'), may hold values from -0.5 to 0.5
- skip_weight: float32 [64, 16], P('tp'), may hold values from -3 to 3
- decay_shift: float32 [64, 32768], P('tp', 'sp'), may hold values from -2 to 0
- head_out_weight: bfloat16 [1024, 2048], P('tp'), may hold values from -0.375 to 0.375
- state_out_weight: bfloat16 [1024, 2048], P('tp'), may hold values from -0.375 to 0.375
Outputs:
- layer_out: bfloat16 [32768, 2048], P('sp', 'tp')
The draws below stay inside these ranges and needn't reach their ends.
All inputs are finite; a program needn't handle non-finite values.
Results may differ from the reference program's by a relative error of at most 0.012.
Values may be sent and summed in bfloat16 or wider, within the bound.
A program may use at most 128 MiB of HBM per device.

```python
import math
import jax
import jax.numpy as jnp
from jax import lax

D = 2048
HEAD_DIM = 64
Q_HEADS = 16
KV_HEADS = 8
SSM_GROUPS = 64
GROUP_CH = 16
SSM_STATE = 64
WINDOW = 128
TOK_DEV = 256
TOKENS = 32768
ATT_WIDTH = 1024
KV_WIDTH = 512
SSM_WIDTH = 1024
N_SP = 128


def group_law(key):
    base_key = jax.random.fold_in(key, 101)
    rank_key, slow_key, fast_key, level_key = jax.random.split(base_key, 4)
    fast_count = SSM_GROUPS // 2
    ranks = jax.random.permutation(rank_key, SSM_GROUPS)
    is_fast = ranks < fast_count
    reach = min(100, TOK_DEV // 2)
    slow_log = jax.random.uniform(slow_key, (SSM_GROUPS,), jnp.float32, math.log(7.0 / TOKENS), math.log(30.0 / TOKENS))
    fast_log = jax.random.uniform(fast_key, (SSM_GROUPS,), jnp.float32, math.log(2.0 / reach), math.log(5.0 / reach))
    log_dt = jnp.where(is_fast, fast_log, slow_log)
    level = jax.random.uniform(level_key, (SSM_GROUPS, SSM_STATE), jnp.float32, 0.3, 0.7)
    slow_real = -level * 0.5 / (jnp.exp(slow_log) * TOKENS)[:, None]
    real_part = jnp.where(is_fast[:, None], -level, slow_real)
    return (log_dt, real_part)


def draw_log_step(key, part):
    return group_law(key)[0]


def draw_decay_real(key, part):
    return group_law(key)[1]


def input_draw(key, salt):
    log_dt, real_part = group_law(key)
    draw_key = jax.random.fold_in(key, salt)
    shape = (SSM_GROUPS, SSM_STATE, GROUP_CH)
    raw = jnp.clip(jax.random.normal(draw_key, shape, jnp.float32), -4.0, 4.0)
    scale = (2.0 * GROUP_CH) ** (-0.5) * jnp.sqrt(2.0 * jnp.abs(real_part) / jnp.exp(log_dt)[:, None])
    return raw * scale[:, :, None]


def draw_input_real(key, part):
    return input_draw(key, 202)


def draw_input_imaginary(key, part):
    return input_draw(key, 203)


def draw_decay_shift(key, part):
    rate_key, jitter_key, where_key, amount_key = jax.random.split(jax.random.fold_in(key, 303), 4)
    block_count = TOKENS // TOK_DEV
    block_rate = jnp.exp(jax.random.uniform(rate_key, (block_count,), jnp.float32, math.log(0.2), math.log(0.8))) / TOKENS
    frequency_ratio = jnp.repeat(block_rate, TOK_DEV)
    random_perturbation = jax.random.uniform(jitter_key, (SSM_GROUPS, TOKENS), jnp.float32, 0.5, 1.5)
    places = jax.random.randint(where_key, (SSM_GROUPS, 2), 0, TOKENS)
    total_quantity = jnp.log(jax.random.uniform(amount_key, (SSM_GROUPS, 2), jnp.float32, 0.5, 0.8))
    positions = jnp.arange(TOKENS, dtype=jnp.int32)
    match_count = (places[:, :, None] == positions[None, None, :]).astype(jnp.float32)
    spike_length = jnp.sum(match_count * total_quantity[:, :, None], axis=1)
    return -frequency_ratio[None, :] * random_perturbation + spike_length


def draw_hidden(key, part):
    noise_key = jax.random.fold_in(jax.random.fold_in(key, 404), 0)
    return jnp.clip(jax.random.normal(noise_key, (TOKENS, D), jnp.float32), -6.0, 6.0).astype(jnp.bfloat16)


def block_scale(rng, dims, shards, least, top_value):
    level, own = 1.0, jax.random.fold_in(rng, 6)
    for position, shards_of in shards:
        draws = jnp.exp(jax.random.uniform(jax.random.fold_in(own, position), (shards_of,), jnp.float32, least / len(shards), top_value / len(shards)))
        level = level * jnp.repeat(draws, dims[position] // shards_of).reshape([-1 if axis == position else 1 for axis in range(len(dims))])
    return level


def gaussian(own_key, shape, width, most, cuts=(), held_as=jnp.bfloat16):
    drawn = jax.random.normal(own_key, shape, jnp.float32) * width
    if len(cuts) > 0:
        drawn = block_scale(own_key, shape, cuts, -0.22, 0.18) * drawn
    return jnp.clip(drawn, min=-most, max=most).astype(held_as)


def setup_inputs(seed: int = 0) -> dict:
    key_of = jax.random.split(jax.random.key(seed), 20)
    return {
        "hidden": draw_hidden(jax.random.fold_in(key_of[19], 71), 0),
        "query_weight": gaussian(key_of[1], (D, ATT_WIDTH), D ** -0.5, 0.125, ((1, 2),)),
        "key_weight": gaussian(key_of[2], (D, KV_WIDTH), D ** -0.5, 0.125, ((1, 2),)),
        "value_weight": gaussian(key_of[3], (D, KV_WIDTH), D ** -0.5, 0.125, ((1, 2),)),
        "head_gate_weight": gaussian(key_of[4], (D, ATT_WIDTH), D ** -0.5, 0.125, ((1, 2),)),
        "state_in_weight": gaussian(key_of[5], (D, SSM_WIDTH), D ** -0.5, 0.125, ((1, 2),)),
        "state_gate_weight": gaussian(key_of[6], (D, SSM_WIDTH), D ** -0.5, 0.125, ((1, 2),)),
        "sink_logit": jnp.clip(1.0 + 5.0 * jax.random.uniform(key_of[7], (Q_HEADS,), jnp.float32) ** block_scale(key_of[7], (Q_HEADS,), ((0, 2),), -0.2, 0.2), 1.0, 6.0),
        "decay_real": draw_decay_real(jax.random.fold_in(key_of[19], 71), 0),
        "decay_frequency": jnp.clip(192.0 * jax.random.uniform(key_of[9], (SSM_GROUPS, SSM_STATE), jnp.float32) ** block_scale(key_of[9], (SSM_GROUPS, SSM_STATE), ((0, 2),), -0.2, 0.2), 0.0, 192.0),
        "log_step": draw_log_step(jax.random.fold_in(key_of[19], 71), 0),
        "input_real": draw_input_real(jax.random.fold_in(key_of[19], 71), 0),
        "input_imaginary": draw_input_imaginary(jax.random.fold_in(key_of[19], 71), 0),
        "output_real": gaussian(key_of[13], (SSM_GROUPS, GROUP_CH, SSM_STATE), (2 * SSM_STATE) ** -0.5, 0.5, ((0, 2),), jnp.float32),
        "output_imaginary": gaussian(key_of[14], (SSM_GROUPS, GROUP_CH, SSM_STATE), (2 * SSM_STATE) ** -0.5, 0.5, ((0, 2),), jnp.float32),
        "skip_weight": gaussian(key_of[15], (SSM_GROUPS, GROUP_CH), 0.5, 3.0, ((0, 2),), jnp.float32),
        "decay_shift": draw_decay_shift(jax.random.fold_in(key_of[19], 71), 0),
        "head_out_weight": gaussian(key_of[17], (ATT_WIDTH, D), (ATT_WIDTH // 4) ** -0.5, 0.375, ((0, 2),)),
        "state_out_weight": gaussian(key_of[18], (SSM_WIDTH, D), (SSM_WIDTH // 4) ** -0.5, 0.375, ((0, 2),)),
    }


NEG_FILL = -1e30


def combine(earlier_pair, later_pair):
    prior_real, prior_imag, prior_sum_real, prior_sum_imag = earlier_pair
    after_real, after_imag, after_sum_real, after_sum_imag = later_pair
    return (prior_real * after_real - prior_imag * after_imag,
            prior_real * after_imag + prior_imag * after_real,
            after_real * prior_sum_real - after_imag * prior_sum_imag + after_sum_real,
            after_real * prior_sum_imag + after_imag * prior_sum_real + after_sum_imag)


def band_rows(rows):
    padded = jnp.concatenate([jnp.zeros_like(rows[:1]), rows], axis=0)
    return jnp.concatenate([padded[:-1], padded[1:]], axis=1)


def attention(query_rows_all, key_rows, value_rows, sink_logit):
    blocks = TOKENS // WINDOW
    group_size = Q_HEADS // KV_HEADS
    query_heads = query_rows_all.reshape(blocks, WINDOW, KV_HEADS, group_size, HEAD_DIM).transpose(2, 0, 1, 3, 4)
    key_heads = band_rows(key_rows.reshape(blocks, WINDOW, KV_HEADS, HEAD_DIM)).transpose(2, 0, 1, 3)
    value_heads = band_rows(value_rows.reshape(blocks, WINDOW, KV_HEADS, HEAD_DIM)).transpose(2, 0, 1, 3)
    sink_table = sink_logit.reshape(KV_HEADS, group_size)
    query_index = jnp.arange(WINDOW, dtype=jnp.int32)[:, None]
    column = jnp.arange(2 * WINDOW, dtype=jnp.int32)[None, :]
    distance = WINDOW + query_index - column
    block_start = (jnp.arange(blocks, dtype=jnp.int32) * WINDOW)[:, None, None]
    allowed = (distance >= 0) & (distance < WINDOW) & (block_start - WINDOW + column >= 0)

    def one_head(operands):
        query_part, key_portion_slice, value_part, sink_part = operands
        scores = jnp.einsum('nqgd,nsd->ngqs', query_part.astype(jnp.float32),
                            key_portion_slice.astype(jnp.float32)) * (HEAD_DIM ** -0.5)
        scores = jnp.where(allowed[:, None], scores, NEG_FILL)
        sink_col = sink_part[None, :, None, None]
        maxima = jnp.maximum(jnp.max(scores, axis=-1, keepdims=True), sink_col)
        exponent = jnp.exp(scores - maxima)
        totals = jnp.sum(exponent, axis=-1, keepdims=True) + jnp.exp(sink_col - maxima)
        weights = (exponent / totals).astype(jnp.bfloat16)
        return jnp.einsum('ngqs,nsd->nqgd', weights.astype(jnp.float32), value_part.astype(jnp.float32))

    outputs = lax.map(one_head, (query_heads, key_heads, value_heads, sink_table))
    return outputs.transpose(1, 2, 0, 3, 4).reshape(TOKENS, ATT_WIDTH)


def state_branch(state_input, decay_real, decay_frequency, log_step, input_real, input_imaginary,
                 output_real, output_imaginary, skip_weight, decay_shift):
    highest = lax.Precision.HIGHEST
    stepsize = jnp.exp(log_step)[:, None]
    magnitude = jnp.exp(decay_real * stepsize)
    base_real = magnitude * jnp.cos(decay_frequency * stepsize)
    base_imag = magnitude * jnp.sin(decay_frequency * stepsize)
    denominator = decay_real * decay_real + decay_frequency * decay_frequency
    less_real = base_real - 1.0
    zoh_real = (less_real * decay_real + base_imag * decay_frequency) / denominator
    zoh_imag = (base_imag * decay_real - less_real * decay_frequency) / denominator
    drive_real = zoh_real[..., None] * input_real - zoh_imag[..., None] * input_imaginary
    drive_imag = zoh_real[..., None] * input_imaginary + zoh_imag[..., None] * input_real
    values = state_input.astype(jnp.float32).reshape(N_SP, TOK_DEV, SSM_GROUPS, GROUP_CH)
    shifts = decay_shift.reshape(SSM_GROUPS, N_SP, TOK_DEV).transpose(1, 0, 2)

    def advance(carried, operands):
        carry_real, carry_imag = carried
        block_rows, shift_rows = operands
        push_real = jnp.einsum('tgp,gnp->gnt', block_rows, drive_real, precision=highest)
        push_imag = jnp.einsum('tgp,gnp->gnt', block_rows, drive_imag, precision=highest)
        factor = jnp.exp(shift_rows)[:, None, :]
        cum_real, cum_imag, local_real, local_imag = lax.associative_scan(
            combine, (factor * base_real[..., None], factor * base_imag[..., None], push_real, push_imag), axis=2)
        state_real = local_real + cum_real * carry_real[..., None] - cum_imag * carry_imag[..., None]
        state_imag = local_imag + cum_real * carry_imag[..., None] + cum_imag * carry_real[..., None]
        recurrent = (jnp.einsum('gpn,gnt->tgp', output_real, state_real, precision=highest)
                     - jnp.einsum('gpn,gnt->tgp', output_imaginary, state_imag, precision=highest)
                     + skip_weight[None] * block_rows)
        return (state_real[..., -1], state_imag[..., -1]), recurrent

    zero_state = jnp.zeros((SSM_GROUPS, SSM_STATE), jnp.float32)
    _, outputs = lax.scan(advance, (zero_state, zero_state), (values, shifts))
    return outputs.reshape(TOKENS, SSM_WIDTH)


def reference(hidden, query_weight, key_weight, value_weight, head_gate_weight, state_in_weight,
              state_gate_weight, sink_logit, decay_real, decay_frequency, log_step, input_real,
              input_imaginary, output_real, output_imaginary, skip_weight, decay_shift,
              head_out_weight, state_out_weight):
    def project(weight):
        return jnp.dot(hidden, weight, preferred_element_type=jnp.float32).astype(jnp.bfloat16)

    query_rows_all = project(query_weight)
    key_rows = project(key_weight)
    value_rows = project(value_weight)
    head_gate = project(head_gate_weight)
    state_input = project(state_in_weight)
    state_gate = project(state_gate_weight)
    attended = attention(query_rows_all, key_rows, value_rows, sink_logit)
    head_mixed = (jax.nn.sigmoid(head_gate.astype(jnp.float32)) * attended).astype(jnp.bfloat16)
    recurrent = state_branch(state_input, decay_real, decay_frequency, log_step, input_real,
                             input_imaginary, output_real, output_imaginary, skip_weight, decay_shift)
    state_mixed = (jax.nn.sigmoid(state_gate.astype(jnp.float32)) * jax.nn.gelu(recurrent)).astype(jnp.bfloat16)
    totals = (jnp.dot(head_mixed, head_out_weight, preferred_element_type=jnp.float32)
              + jnp.dot(state_mixed, state_out_weight, preferred_element_type=jnp.float32))
    return totals.astype(jnp.bfloat16)
```

```python
import functools

import jax
import jax.numpy as jnp
from jax import lax
from jax.experimental import pallas as pl
from jax.experimental.pallas import tpu as pltpu
from jax.sharding import PartitionSpec as P

MESH = pl.DeviceIdType.MESH
F32 = jnp.float32
BF16 = jnp.bfloat16

TOK = 256
D = 2048
HALF = D // 2
WINDOW = 128
SEG = 16
CHUNKS = TOK // SEG
PAIRS = 16
LANES = PAIRS * 256
KV_HEADS = 4
SP_SIZES = {128: (8, 4, 4), 8: (2, 2, 2)}

HID, HALO, OUT = 0, 1, 2
N_OUT = 4


def dot(a, b):
    return jnp.dot(a, b, preferred_element_type=F32)


def dot_nt(a, b):
    return lax.dot_general(a, b, (((1,), (1,)), ((), ())), preferred_element_type=F32)


def cmul(a, b):
    return (a[0] * b[0] - a[1] * b[1], a[0] * b[1] + a[1] * b[0])


def csquares(a, times):
    for _ in range(times):
        a = cmul(a, a)
    return a


def log2(n):
    return n.bit_length() - 1


def kernel(
    sizes,
    hidden,
    w_query,
    w_key,
    w_value,
    w_hgate,
    w_sin,
    w_sgate,
    w_hout,
    w_sout,
    sink,
    base,
    drive_c,
    out_c,
    skip,
    shift,
    out,
    h_ref,
    win,
    wkv,
    wq,
    whg,
    wsg,
    who,
    wso,
    drive,
    cmat,
    tri,
    grow,
    shrink,
    decay,
    shift_tile,
    u_ref,
    us_ref,
    es_ref,
    x_ref,
    s_ref,
    tot_re,
    tot_im,
    ent_re,
    ent_im,
    q_ref,
    kv_ref,
    hg_ref,
    sg_ref,
    hm_ref,
    sm_ref,
    acc_ref,
    psend,
    precv,
    own_x,
    own_y,
    own_z,
    got_x,
    got_y,
    got_z,
    pre_z,
    w_sem,
    send_sem,
    recv_sem,
):
    nz, ny, nx = sizes
    n_sp = nz * ny * nx
    sp, tp = lax.axis_index("sp"), lax.axis_index("tp")
    z, y, x = sp // (ny * nx), (sp // nx) % ny, sp % nx
    other = 1 - tp
    nxt, prv = lax.rem(sp + 1, n_sp), lax.rem(sp + n_sp - 1, n_sp)

    loads = []

    def load(src, dst):
        copy = pltpu.make_async_copy(src, dst, w_sem.at[len(loads)])
        copy.start()
        loads.append(copy)
        return copy

    mine = pl.ds(pl.multiple_of(tp * HALF, HALF), HALF)
    theirs = pl.ds(pl.multiple_of(other * HALF, HALF), HALF)
    l_h = load(hidden, h_ref.at[:, mine])
    l_in = load(w_sin, win)
    l_k = load(w_key, wkv.at[:, 0:256])
    l_v = load(w_value, wkv.at[:, 256:512])
    l_q = load(w_query, wq)
    l_hg = load(w_hgate, whg)
    l_sg = load(w_sgate, wsg)
    l_ho = load(w_hout, who)
    l_so = load(w_sout, wso)

    def x_peer(r):
        return (sp - x + lax.rem(x + r, nx), tp)

    def y_peer(r):
        return (sp + (lax.rem(y + r, ny) - y) * nx, tp)

    def z_peer(r):
        return (sp + (lax.rem(z + r, nz) - z) * (nx * ny), tp)

    peers = [(sp, other), (nxt, tp), (prv, tp)]
    peers += [x_peer(r) for r in range(1, nx)]
    peers += [y_peer(r) for r in range(1, ny)]
    peers += [z_peer(r) for r in range(1, nz)]
    barrier = pltpu.get_barrier_semaphore()
    for peer in peers:
        pl.semaphore_signal(barrier, inc=1, device_id=peer, device_id_type=MESH)

    def remote(src, dst, number, device):
        return pltpu.make_async_remote_copy(
            src_ref=src,
            dst_ref=dst,
            send_sem=send_sem.at[number],
            recv_sem=recv_sem.at[number],
            device_id=device,
            device_id_type=MESH,
        )

    row = lax.broadcasted_iota(jnp.int32, (TOK, TOK), 0)
    col = lax.broadcasted_iota(jnp.int32, (TOK, TOK), 1)
    tri[0:TOK, :] = ((row // SEG == col // SEG) & (col <= row)).astype(F32).astype(BF16)
    srow = lax.broadcasted_iota(jnp.int32, (CHUNKS, TOK), 0)
    scol = lax.broadcasted_iota(jnp.int32, (CHUNKS, TOK), 1)
    tri[TOK:, :] = (scol // SEG == srow).astype(F32).astype(BF16)
    drive[...] = jnp.zeros_like(drive)
    cmat[...] = jnp.zeros_like(cmat)
    for i in range(PAIRS):
        rows, cols = slice((i % 4) * 32, (i % 4) * 32 + 32), slice(i * 256, i * 256 + 256)
        drive[rows, cols] = drive_c[i * 32 : i * 32 + 32, :]
        cmat[rows, cols] = out_c[i * 32 : i * 32 + 32, :]

    power = lax.broadcasted_iota(jnp.int32, (8, 128), 0) + 1
    ones, zeros = jnp.ones((8, 128), F32), jnp.zeros((8, 128), F32)
    for table, first in ((grow, 0), (shrink, 2)):
        for i in range(PAIRS):
            b = tuple(jnp.broadcast_to(base[first + k, i : i + 1, :], (8, 128)) for k in (0, 1))
            value = (ones, zeros)
            for bit in range(4):
                has = (power >> bit) & 1 == 1
                value = cmul(value, (jnp.where(has, b[0], ones), jnp.where(has, b[1], zeros)))
                if bit < 3:
                    b = cmul(b, b)
            cols = slice(i * 128, i * 128 + 128)
            upper = cmul(value, b)
            for k in (0, 1):
                table[k, 0:8, cols] = value[k]
                table[k, 8:16, cols] = upper[k]
    a_seg = csquares((base[0], base[1]), log2(SEG))
    a_dev = csquares(a_seg, log2(CHUNKS))
    a_line = csquares(a_dev, log2(nx))
    a_plane = csquares(a_line, log2(ny))

    rest = jnp.broadcast_to(shift[...][:, None, :], (2 * PAIRS, 16, TOK)).reshape(512, TOK)
    sums = None
    for k in range(3):
        part = rest.astype(BF16)
        term = dot_nt(tri[0:TOK, :], part)
        sums = term if sums is None else sums + term
        rest = rest - part.astype(F32)
    es_ref[...] = sums
    low = lax.broadcasted_iota(jnp.int32, (PAIRS, 128), 1) < 64
    lane = lax.broadcasted_iota(jnp.int32, (PAIRS, 128), 1)
    total_shift = jnp.zeros((PAIRS, 128), F32)
    for c in range(CHUNKS):
        if c % 8 == 0:
            shift_tile[...] = shift[:, c * SEG : c * SEG + 128]
            even = shift_tile[pl.ds(0, PAIRS, stride=2), :]
            odd = shift_tile[pl.ds(1, PAIRS, stride=2), :]
        inside = lane // SEG == c % 8
        s = jnp.where(
            low,
            jnp.sum(jnp.where(inside, even, 0.0), axis=1, keepdims=True),
            jnp.sum(jnp.where(inside, odd, 0.0), axis=1, keepdims=True),
        )
        total_shift = total_shift + s
        decay[c] = jnp.exp(s)

    pl.semaphore_wait(barrier, len(peers))
    send_h = remote(hidden, h_ref.at[:, mine], HID, (sp, other))
    send_h.start()

    l_h.wait()
    l_in.wait()
    u_ref[...] = dot(h_ref[:, mine], win[mine, :])
    send_h.wait_recv()
    u = (u_ref[...] + dot(h_ref[:, theirs], win[theirs, :])).astype(BF16).astype(F32)
    u_ref[...] = u
    us_ref[...] = (u * jnp.exp(-es_ref[...])).astype(BF16)

    for i in range(PAIRS):
        cols, narrow = slice(i * 256, i * 256 + 256), slice(i * 128, i * 128 + 128)
        j = i // 4
        push = dot(us_ref[:, j * 128 : j * 128 + 128], drive[:, cols])
        push = (push[:, :128].reshape(CHUNKS, SEG, 128), push[:, 128:].reshape(CHUNKS, SEG, 128))
        back = (shrink[0, :, narrow][None], shrink[1, :, narrow][None])
        w = cmul(push, back)
        w = jnp.concatenate([part.reshape(TOK, 128).astype(BF16) for part in w], axis=1)
        summed = dot(tri[...], w)
        x_ref[:, cols] = summed[:TOK]
        tot_re[i * 16 : i * 16 + 16, :] = summed[TOK:, :128]
        tot_im[i * 16 : i * 16 + 16, :] = summed[TOK:, 128:]

    def chunk_scan(state, keep):
        for c in range(CHUNKS):
            at = pl.ds(c, PAIRS, stride=CHUNKS)
            if keep:
                ent_re[at, :] = state[0]
                ent_im[at, :] = state[1]
            e = decay[c]
            state = cmul(
                (state[0] + tot_re[at, :], state[1] + tot_im[at, :]), (a_seg[0] * e, a_seg[1] * e)
            )
        return state

    flat_zero = jnp.zeros((PAIRS, 128), F32)
    flat_one = jnp.ones((PAIRS, 128), F32)
    local = chunk_scan((flat_zero, flat_zero), False)
    own_x[0], own_x[1], own_x[2] = local[0], local[1], total_shift
    number = OUT + N_OUT
    sends_x = []
    for r in range(1, nx):
        copy = remote(own_x, got_x.at[r - 1], number, x_peer(r))
        copy.start()
        sends_x.append(copy)
        number += 1

    l_k.wait()
    l_v.wait()
    kv_ref[WINDOW:, :] = dot(h_ref[...], wkv[...]).astype(BF16)
    halo = remote(kv_ref.at[TOK : TOK + WINDOW, :], kv_ref.at[0:WINDOW, :], HALO, (nxt, tp))
    l_q.wait()
    q_ref[...] = (dot(h_ref[...], wq[...]).astype(BF16).astype(F32) * 0.125)
    halo.start()

    def stage(got, own, a, at, count):
        factors = []
        for r in range(1, count):
            e = jnp.exp(got[r - 1, 2])
            factors.append((a[0] * e, a[1] * e))
        before, through = (flat_zero, flat_zero), (flat_one, flat_zero)
        total_s = own[2]
        for r in range(count - 1, 0, -1):
            earlier = r <= at
            f = factors[r - 1]
            new = cmul(f, before)
            before = (
                jnp.where(earlier, new[0] + got[r - 1, 0], before[0]),
                jnp.where(earlier, new[1] + got[r - 1, 1], before[1]),
            )
            new = cmul(f, through)
            through = (
                jnp.where(earlier, new[0], through[0]),
                jnp.where(earlier, new[1], through[1]),
            )
            total_s = total_s + got[r - 1, 2]
        e = jnp.exp(own[2])
        new = cmul((a[0] * e, a[1] * e), before)
        total = (new[0] + own[0], new[1] + own[1])
        for r in range(count - 1, 0, -1):
            later = r > at
            new = cmul(factors[r - 1], total)
            total = (
                jnp.where(later, new[0] + got[r - 1, 0], total[0]),
                jnp.where(later, new[1] + got[r - 1, 1], total[1]),
            )
        return before, through, total, total_s

    for copy in sends_x:
        copy.wait_recv()
    before_x, through_x, total, total_s = stage(got_x, own_x, a_dev, x, nx)
    own_y[0], own_y[1], own_y[2] = total[0], total[1], total_s
    sends_y = []
    for r in range(1, ny):
        copy = remote(own_y, got_y.at[r - 1], number, y_peer(r))
        copy.start()
        sends_y.append(copy)
        number += 1

    l_hg.wait()
    hg_ref[...] = dot(h_ref[...], whg[...]).astype(BF16).astype(F32)
    l_sg.wait()
    sg_ref[...] = dot(h_ref[...], wsg[...]).astype(BF16).astype(F32)

    for copy in sends_y:
        copy.wait_recv()
    before_y, through_y, total, total_s = stage(got_y, own_y, a_line, y, ny)
    own_z[0], own_z[1], own_z[2] = total[0], total[1], total_s
    sends_z = []
    for r in range(1, nz):
        copy = remote(own_z, got_z.at[r - 1], number, z_peer(r))
        pl.when(z + r < nz)(copy.start)
        sends_z.append(copy)
        number += 1

    halo.wait_recv()
    qi = lax.rem(lax.broadcasted_iota(jnp.int32, (2 * WINDOW, 2 * WINDOW), 0), WINDOW)
    key_at = lax.broadcasted_iota(jnp.int32, (2 * WINDOW, 2 * WINDOW), 1)
    inside = (key_at > qi) & (key_at <= qi + WINDOW)
    left = lax.broadcasted_iota(jnp.int32, (WINDOW, 128), 1) < 64
    for n in range(TOK // WINDOW):
        allowed = inside & ((key_at >= WINDOW) | (sp > 0)) if n == 0 else inside
        rows = slice(n * WINDOW, (n + 1) * WINDOW)
        keys = slice(n * WINDOW, (n + 2) * WINDOW)
        for h in range(KV_HEADS):
            q = q_ref[rows, h * 128 : h * 128 + 128]
            turned = pltpu.roll(q, 64, 1)
            in_half = left if h % 2 == 0 else jnp.logical_not(left)
            first, second = (q, turned) if h % 2 == 0 else (turned, q)
            stacked = jnp.concatenate(
                [jnp.where(in_half, part, 0.0).astype(BF16) for part in (first, second)], axis=0
            )
            tile = slice((h // 2) * 128, (h // 2) * 128 + 128)
            scores = dot_nt(stacked, kv_ref[keys, tile])
            scores = jnp.where(allowed, scores, -1e30)
            first_row = lax.broadcasted_iota(jnp.int32, (2 * WINDOW, 1), 0) < WINDOW
            sink_col = jnp.where(first_row, sink[2 * h], sink[2 * h + 1])
            peak = jnp.maximum(jnp.max(scores, axis=1, keepdims=True), sink_col)
            e = jnp.exp(scores - peak)
            total = jnp.sum(e, axis=1, keepdims=True) + jnp.exp(sink_col - peak)
            vtile = slice(256 + (h // 2) * 128, 256 + (h // 2) * 128 + 128)
            mixed = dot(e.astype(BF16), kv_ref[keys, vtile]) / total
            a, b = mixed[:WINDOW], mixed[WINDOW:]
            if h % 2 == 0:
                joined = jnp.where(left, a, pltpu.roll(b, 64, 1))
            else:
                joined = jnp.where(left, pltpu.roll(a, 64, 1), b)
            gate = jax.nn.sigmoid(hg_ref[rows, h * 128 : h * 128 + 128])
            hm_ref[rows, h * 128 : h * 128 + 128] = (gate * joined).astype(BF16)
    l_ho.wait()
    acc_ref[...] = dot(hm_ref[...], who[...])

    pre_z[...] = jnp.zeros_like(pre_z)
    for r in range(nz - 1, 0, -1):

        @pl.when(r <= z)
        def _(r=r):
            sends_z[r - 1].wait_recv()
            e = jnp.exp(got_z[r - 1, 2])
            new = cmul((a_plane[0] * e, a_plane[1] * e), (pre_z[0], pre_z[1]))
            pre_z[0] = new[0] + got_z[r - 1, 0]
            pre_z[1] = new[1] + got_z[r - 1, 1]

    carry = cmul(through_y, (pre_z[0], pre_z[1]))
    carry = cmul(through_x, (before_y[0] + carry[0], before_y[1] + carry[1]))
    chunk_scan((before_x[0] + carry[0], before_x[1] + carry[1]), True)

    for j in range(4):
        for k in range(4):
            i = 4 * j + k
            narrow = slice(i * 128, i * 128 + 128)
            state = tuple(
                x_ref[:, i * 256 + 128 * part : i * 256 + 128 * part + 128].reshape(CHUNKS, SEG, 128)
                + entry[i * 16 : i * 16 + 16, :][:, None, :]
                for part, entry in ((0, ent_re), (1, ent_im))
            )
            state = cmul(state, (grow[0, :, narrow][None], grow[1, :, narrow][None]))
            s_ref[:, k * 256 : k * 256 + 128] = state[0].reshape(TOK, 128).astype(BF16)
            s_ref[:, k * 256 + 128 : k * 256 + 256] = state[1].reshape(TOK, 128).astype(BF16)
        cols = slice(j * 128, j * 128 + 128)
        rec = dot_nt(s_ref[...], cmat[:, j * 1024 : j * 1024 + 1024])
        rec = rec * jnp.exp(es_ref[:, cols]) + skip[:, cols] * u_ref[:, cols]
        gate = jax.nn.sigmoid(sg_ref[:, cols])
        sm_ref[:, cols] = (gate * jax.nn.gelu(rec)).astype(BF16)

    l_so.wait()
    outs = []
    for k in range(N_OUT):
        cols = pl.ds(pl.multiple_of(other * HALF + k * 256, 256), 256)
        psend[k] = (acc_ref[:, cols] + dot(sm_ref[...], wso[:, cols])).astype(BF16)
        copy = remote(psend.at[k], precv.at[k], OUT + k, (sp, other))
        copy.start()
        outs.append(copy)
    for k in range(N_OUT):
        cols = pl.ds(pl.multiple_of(tp * HALF + k * 256, 256), 256)
        own = acc_ref[:, cols] + dot(sm_ref[...], wso[:, cols])
        outs[k].wait_recv()
        out[:, k * 256 : k * 256 + 256] = (own + precv[k].astype(F32)).astype(BF16)

    send_h.wait_send()
    halo.wait_send()
    for copy in sends_x + sends_y + outs:
        copy.wait_send()
    for r in range(1, nz):
        pl.when(z + r < nz)(sends_z[r - 1].wait_send)


def placed(re, im):
    groups, rows, states = re.shape
    re = re.reshape(groups // 2, 2, rows, states)
    im = im.reshape(groups // 2, 2, rows, states)
    none = jnp.zeros_like(re[:, 0])
    even = jnp.concatenate([re[:, 0], none, im[:, 0], none], axis=-1)
    odd = jnp.concatenate([none, re[:, 1], none, im[:, 1]], axis=-1)
    return jnp.stack([even, odd], axis=1).reshape(groups * rows, 4 * states).astype(BF16)


def on_device(
    sizes,
    hidden,
    query_weight,
    key_weight,
    value_weight,
    head_gate_weight,
    state_in_weight,
    state_gate_weight,
    sink_logit,
    decay_real,
    decay_frequency,
    log_step,
    input_real,
    input_imaginary,
    output_real,
    output_imaginary,
    skip_weight,
    decay_shift,
    head_out_weight,
    state_out_weight,
):
    nz, ny, nx = sizes
    stepsize = jnp.exp(log_step)[:, None]
    log_magnitude = decay_real * stepsize
    rotation = decay_frequency * stepsize
    magnitude, inverse = jnp.exp(log_magnitude), jnp.exp(-log_magnitude)
    cosine, sine = jnp.cos(rotation), jnp.sin(rotation)
    base_real, base_imag = magnitude * cosine, magnitude * sine
    denominator = decay_real * decay_real + decay_frequency * decay_frequency
    less_real = base_real - 1.0
    zoh_real = ((less_real * decay_real + base_imag * decay_frequency) / denominator)[:, None, :]
    zoh_imag = ((base_imag * decay_real - less_real * decay_frequency) / denominator)[:, None, :]
    in_real, in_imag = input_real.transpose(0, 2, 1), input_imaginary.transpose(0, 2, 1)
    drive = placed(
        zoh_real * in_real - zoh_imag * in_imag, zoh_real * in_imag + zoh_imag * in_real
    )
    outm = placed(output_real, -output_imaginary)
    base = jnp.stack([base_real, base_imag, inverse * cosine, -inverse * sine]).reshape(
        4, PAIRS, 128
    )
    skip = skip_weight.reshape(1, 512)

    vmem = pl.BlockSpec(memory_space=pltpu.VMEM)
    hbm = pl.BlockSpec(memory_space=pl.ANY)
    n_remote = OUT + N_OUT + (nx - 1) + (ny - 1) + (nz - 1)
    scratch = [
        ((TOK, D), BF16),
        ((D, 512), BF16),
        ((D, 512), BF16),
        ((D, 512), BF16),
        ((D, 512), BF16),
        ((D, 512), BF16),
        ((512, D), BF16),
        ((512, D), BF16),
        ((128, LANES), BF16),
        ((128, LANES), BF16),
        ((TOK + CHUNKS, TOK), BF16),
        ((2, SEG, PAIRS * 128), F32),
        ((2, SEG, PAIRS * 128), F32),
        ((CHUNKS, PAIRS, 128), F32),
        ((2 * PAIRS, 128), F32),
        ((TOK, 512), F32),
        ((TOK, 512), BF16),
        ((TOK, 512), F32),
        ((TOK, LANES), F32),
        ((TOK, 1024), BF16),
        ((PAIRS * CHUNKS, 128), F32),
        ((PAIRS * CHUNKS, 128), F32),
        ((PAIRS * CHUNKS, 128), F32),
        ((PAIRS * CHUNKS, 128), F32),
        ((TOK, 512), F32),
        ((TOK + WINDOW, 512), BF16),
        ((TOK, 512), F32),
        ((TOK, 512), F32),
        ((TOK, 512), BF16),
        ((TOK, 512), BF16),
        ((TOK, D), F32),
        ((N_OUT, TOK, 256), BF16),
        ((N_OUT, TOK, 256), BF16),
        ((3, PAIRS, 128), F32),
        ((3, PAIRS, 128), F32),
        ((3, PAIRS, 128), F32),
        ((nx - 1, 3, PAIRS, 128), F32),
        ((ny - 1, 3, PAIRS, 128), F32),
        ((nz - 1, 3, PAIRS, 128), F32),
        ((2, PAIRS, 128), F32),
    ]
    return pl.pallas_call(
        functools.partial(kernel, sizes),
        out_shape=jax.ShapeDtypeStruct((TOK, HALF), BF16),
        in_specs=[hbm] * 9 + [pl.BlockSpec(memory_space=pltpu.SMEM)] + [vmem] * 5,
        out_specs=vmem,
        scratch_shapes=[pltpu.VMEM(shape, dtype) for shape, dtype in scratch]
        + [
            pltpu.SemaphoreType.DMA((9,)),
            pltpu.SemaphoreType.DMA((n_remote,)),
            pltpu.SemaphoreType.DMA((n_remote,)),
        ],
        compiler_params=pltpu.CompilerParams(
            collective_id=0, has_side_effects=True, vmem_limit_bytes=60 * 1024 * 1024
        ),
        name="layer",
    )(
        hidden,
        query_weight,
        key_weight,
        value_weight,
        head_gate_weight,
        state_in_weight,
        state_gate_weight,
        head_out_weight,
        state_out_weight,
        sink_logit,
        base,
        drive,
        outm,
        skip,
        decay_shift,
    )


def solution(mesh):
    sizes = SP_SIZES[mesh.shape["sp"]]
    in_specs = (
        P("sp", "tp"),
        P(None, "tp"),
        P(None, "tp"),
        P(None, "tp"),
        P(None, "tp"),
        P(None, "tp"),
        P(None, "tp"),
        P("tp"),
        P("tp", None),
        P("tp", None),
        P("tp"),
        P("tp", None, None),
        P("tp", None, None),
        P("tp", None, None),
        P("tp", None, None),
        P("tp", None),
        P("tp", "sp"),
        P("tp", None),
        P("tp", None),
    )
    return jax.shard_map(
        functools.partial(on_device, sizes),
        mesh=mesh,
        in_specs=in_specs,
        out_specs=P("sp", "tp"),
        check_vma=False,
    )
```

```python
import functools

import jax
import jax.numpy as jnp
from jax import lax
from jax.experimental import pallas as pl
from jax.experimental.pallas import tpu as pltpu
from jax.sharding import PartitionSpec as P

MESH = pl.DeviceIdType.MESH
F32 = jnp.float32
BF16 = jnp.bfloat16

TOK = 256
D = 2048
HALF = D // 2
WINDOW = 128
SEG = 16
CHUNKS = TOK // SEG
PAIRS = 16
LANES = PAIRS * 256
KV_HEADS = 4
SP_SIZES = {128: (8, 4, 4), 8: (2, 2, 2)}

N_OUT = 4


def dot(a, b):
    return jnp.dot(a, b, preferred_element_type=F32)


def dot_nt(a, b):
    return lax.dot_general(a, b, (((1,), (1,)), ((), ())), preferred_element_type=F32)


def cmul(a, b):
    return (a[0] * b[0] - a[1] * b[1], a[0] * b[1] + a[1] * b[0])


def csquares(a, times):
    for _ in range(times):
        a = cmul(a, a)
    return a


def log2(n):
    return n.bit_length() - 1


def kernel(sizes, *refs):
    nz, ny, nx = sizes
    plane = ny * nx
    (
        hidden,
        w_query,
        w_key,
        w_value,
        w_hgate,
        w_sin,
        w_sgate,
        w_hout,
        w_sout,
        sink_in,
        step_in,
        real_in,
        freq_in,
        in_re_in,
        in_im_in,
        out_re_in,
        out_im_in,
        skip_in,
        shift_in,
        out,
        sink,
        log_step,
        decay_real,
        decay_freq,
        in_re,
        in_im,
        out_re,
        out_im,
        skip_t,
        shift,
        h_ref,
        win,
        wkv,
        wq,
        whg,
        wsg,
        who,
        wso,
        drive,
        cmat,
        mmat,
        c_ref,
        tri,
        grow,
        shrink,
        decay,
        pair_tile,
        u_ref,
        us_ref,
        es_ref,
        ed_ref,
        w_ref,
        s_ref,
        g_ref,
        yl_ref,
        tot_re,
        tot_im,
        ent_re,
        ent_im,
        pow_re,
        pow_im,
        q_ref,
        kv_ref,
        hg_ref,
        sg_ref,
        hm_ref,
        sm_ref,
        acc_ref,
        psend,
        precv,
        s_buf,
        l_buf,
        zs_buf,
        zl_buf,
        pre,
        load_sem,
        h_sem,
        halo_sem,
        out_send,
        out_recv,
        s_send,
        s_recv,
        l_send,
        l_recv,
        zs_send,
        zs_recv,
        zl_send,
        zl_recv,
        ready_plane,
        ready_z,
        ready_halo,
    ) = refs
    sp, tp = lax.axis_index("sp"), lax.axis_index("tp")
    z, m = sp // plane, sp % plane
    other = 1 - tp

    loads = []

    def load(src, dst):
        copy = pltpu.make_async_copy(src, dst, load_sem.at[len(loads)])
        copy.start()
        loads.append(copy)
        return copy

    def remote(src, dst, send, recv, device):
        return pltpu.make_async_remote_copy(
            src_ref=src,
            dst_ref=dst,
            send_sem=send,
            recv_sem=recv,
            device_id=device,
            device_id_type=MESH,
        )

    mine = pl.ds(pl.multiple_of(tp * HALF, HALF), HALF)
    theirs = pl.ds(pl.multiple_of(other * HALF, HALF), HALF)
    l_h = load(hidden, h_ref.at[:, mine])
    small = [
        load(src, dst)
        for src, dst in (
            (step_in, log_step),
            (real_in, decay_real),
            (freq_in, decay_freq),
            (shift_in, shift),
            (in_re_in, in_re),
            (in_im_in, in_im),
            (out_re_in, out_re),
            (out_im_in, out_im),
            (skip_in, skip_t),
            (sink_in, sink),
        )
    ]
    l_in = load(w_sin, win)

    barrier = pltpu.get_barrier_semaphore()

    def signal(semaphore, device):
        pl.semaphore_signal(semaphore, inc=1, device_id=device, device_id_type=MESH)

    def when(condition, act, *args):
        pl.when(condition)(functools.partial(act, *args))

    crosses = jnp.logical_and(m == plane - 1, z < nz - 1)
    crossed = jnp.logical_and(m == 0, z > 0)
    signal(barrier, (sp, other))
    for r in range(1, plane):
        when(m + r < plane, signal, barrier, (sp + r, tp))
    for r in range(1, nz):
        when(z + r < nz, signal, barrier, (sp + r * plane, tp))
    when(crosses, signal, barrier, (sp + 1, tp))
    pl.semaphore_wait(barrier, 1 + m + z + crossed.astype(jnp.int32))
    l_h.wait()
    send_h = remote(h_ref.at[:, mine], h_ref.at[:, mine], h_sem.at[0], h_sem.at[1], (sp, other))
    send_h.start()
    for r in range(1, plane):
        when(m >= r, signal, ready_plane, (sp - r, tp))
    for r in range(1, nz):
        when(z >= r, signal, ready_z, (sp - r * plane, tp))
    when(crossed, signal, ready_halo, (sp - 1, tp))
    l_k = load(w_key, wkv.at[:, 0:256])
    l_v = load(w_value, wkv.at[:, 256:512])
    l_q = load(w_query, wq)

    for copy in small:
        copy.wait()
    low = lax.broadcasted_iota(jnp.int32, (PAIRS, 128), 1) < 64

    def paired(value):
        pair_tile[...] = jnp.concatenate([value, value], axis=1)
        even = pair_tile[pl.ds(0, PAIRS, stride=2), :]
        odd = pair_tile[pl.ds(1, PAIRS, stride=2), :]
        return jnp.where(low, even, odd)

    pair_row = lax.broadcasted_iota(jnp.int32, (PAIRS, 128), 0)
    step = jnp.zeros((PAIRS, 128), F32)
    for i in range(PAIRS):
        step = jnp.where(
            pair_row == i, jnp.where(low, log_step[2 * i], log_step[2 * i + 1]), step
        )
    step = jnp.exp(step)
    real, freq = paired(decay_real[...]), paired(decay_freq[...])
    magnitude, inverse = jnp.exp(real * step), jnp.exp(-(real * step))
    cosine, sine = jnp.cos(freq * step), jnp.sin(freq * step)
    base = (magnitude * cosine, magnitude * sine)
    base_inv = (inverse * cosine, -(inverse * sine))
    denominator = real * real + freq * freq
    less = base[0] - 1.0
    zoh = (
        (less * real + base[1] * freq) / denominator,
        (base[1] * real - less * freq) / denominator,
    )

    row = lax.broadcasted_iota(jnp.int32, (TOK, TOK), 0)
    col = lax.broadcasted_iota(jnp.int32, (TOK, TOK), 1)
    tri[0:TOK, :] = ((row // SEG == col // SEG) & (col <= row)).astype(F32).astype(BF16)
    srow = lax.broadcasted_iota(jnp.int32, (CHUNKS, TOK), 0)
    scol = lax.broadcasted_iota(jnp.int32, (CHUNKS, TOK), 1)
    tri[TOK:, :] = (scol // SEG == srow).astype(F32).astype(BF16)
    drive[...] = jnp.zeros_like(drive)
    for i in range(PAIRS):
        factor = (zoh[0][i : i + 1, :], zoh[1][i : i + 1, :])
        first = (i % 4) * 32
        value = cmul(factor, tuple(jnp.concatenate([t[2 * i], t[2 * i + 1]], axis=1) for t in (in_re, in_im)))
        for part in (0, 1):
            cols = slice(i * 256 + part * 128, i * 256 + part * 128 + 128)
            drive[first : first + 16, cols] = jnp.where(low, value[part], 0.0).astype(BF16)
            drive[first + 16 : first + 32, cols] = jnp.where(low, 0.0, value[part]).astype(BF16)

    power = lax.broadcasted_iota(jnp.int32, (8, 128), 0) + 1
    ones, zeros = jnp.ones((8, 128), F32), jnp.zeros((8, 128), F32)
    for table, root in ((grow, base), (shrink, base_inv)):
        for i in range(PAIRS):
            b = tuple(jnp.broadcast_to(part[i : i + 1, :], (8, 128)) for part in root)
            value = (ones, zeros)
            for bit in range(4):
                has = (power >> bit) & 1 == 1
                value = cmul(value, (jnp.where(has, b[0], ones), jnp.where(has, b[1], zeros)))
                if bit < 3:
                    b = cmul(b, b)
            cols = slice(i * 128, i * 128 + 128)
            upper = cmul(value, b)
            for k in (0, 1):
                table[k, 0:8, cols] = value[k]
                table[k, 8:16, cols] = upper[k]
    a_seg = csquares(base, log2(SEG))
    a_dev = csquares(a_seg, log2(CHUNKS))
    a_plane = csquares(a_dev, log2(plane))

    def shift_sums(mask):
        rest = jnp.broadcast_to(shift[...][:, None, :], (2 * PAIRS, 16, TOK)).reshape(512, TOK)
        sums = None
        for _ in range(3):
            part = rest.astype(BF16)
            term = dot_nt(mask, part)
            sums = term if sums is None else sums + term
            rest = rest - part.astype(F32)
        return sums

    es_ref[...] = shift_sums(tri[0:TOK, :])
    lane = lax.broadcasted_iota(jnp.int32, (PAIRS, 128), 1)
    total_shift = jnp.zeros((PAIRS, 128), F32)
    for c in range(CHUNKS):
        if c % 8 == 0:
            pair_tile[...] = shift[:, c * SEG : c * SEG + 128]
            even = pair_tile[pl.ds(0, PAIRS, stride=2), :]
            odd = pair_tile[pl.ds(1, PAIRS, stride=2), :]
        inside = lane // SEG == c % 8
        s = jnp.where(
            low,
            jnp.sum(jnp.where(inside, even, 0.0), axis=1, keepdims=True),
            jnp.sum(jnp.where(inside, odd, 0.0), axis=1, keepdims=True),
        )
        total_shift = total_shift + s
        decay[c] = jnp.exp(s)
    s_buf[m] = total_shift

    l_in.wait()
    u_ref[...] = dot(h_ref[:, mine], win[mine, :])
    send_h.wait_recv()
    l_hg = load(w_hgate, whg)
    l_sg = load(w_sgate, wsg)
    l_ho = load(w_hout, who)
    l_so = load(w_sout, wso)
    u = (u_ref[...] + dot(h_ref[:, theirs], win[theirs, :])).astype(BF16).astype(F32)
    u_ref[...] = u
    us_ref[...] = (u * jnp.exp(-es_ref[...])).astype(BF16)

    when(m < plane - 1, pl.semaphore_wait, ready_plane, plane - 1 - m)

    def plane_copy(buf, send, recv, k):
        return remote(buf.at[m], buf.at[m], send.at[k], recv.at[m], (z * plane + k, tp))

    def plane_wait(buf, send, recv, k):
        remote(buf.at[k], buf.at[k], send.at[k], recv.at[k], (z * plane + k, tp)).wait_recv()

    for k in range(plane):
        when(m != k, plane_copy(s_buf, s_send, s_recv, k).start)

    for i in range(PAIRS):
        cols, narrow = slice(i * 256, i * 256 + 256), slice(i * 128, i * 128 + 128)
        j = i // 4
        push = dot(us_ref[:, j * 128 : j * 128 + 128], drive[:, cols])
        push = (push[:, :128].reshape(CHUNKS, SEG, 128), push[:, 128:].reshape(CHUNKS, SEG, 128))
        back = (shrink[0, :, narrow][None], shrink[1, :, narrow][None])
        w = cmul(push, back)
        w = jnp.concatenate([part.reshape(TOK, 128).astype(BF16) for part in w], axis=1)
        w_ref[:, cols] = w
        summed = dot(tri[TOK:, :], w)
        tot_re[i * 16 : i * 16 + 16, :] = summed[:, :128]
        tot_im[i * 16 : i * 16 + 16, :] = summed[:, 128:]

    flat_zero = jnp.zeros((PAIRS, 128), F32)
    flat_one = jnp.ones((PAIRS, 128), F32)
    state = (flat_zero, flat_zero)
    for c in range(CHUNKS):
        at = pl.ds(c, PAIRS, stride=CHUNKS)
        ent_re[at, :] = state[0]
        ent_im[at, :] = state[1]
        e = decay[c]
        state = cmul(
            (state[0] + tot_re[at, :], state[1] + tot_im[at, :]), (a_seg[0] * e, a_seg[1] * e)
        )
    l_buf[m, 0] = state[0].astype(BF16)
    l_buf[m, 1] = state[1].astype(BF16)
    for k in range(plane):
        when(m != k, plane_copy(l_buf, l_send, l_recv, k).start)

    l_k.wait()
    l_v.wait()
    kv_ref[WINDOW:, :] = dot(h_ref[...], wkv[...]).astype(BF16)
    halo = remote(
        kv_ref.at[TOK : TOK + WINDOW, :],
        kv_ref.at[0:WINDOW, :],
        halo_sem.at[0],
        halo_sem.at[1],
        (lax.rem(sp + 1, nz * plane), tp),
    )
    l_q.wait()
    q_ref[...] = dot(h_ref[...], wq[...]).astype(BF16).astype(F32) * 0.125
    when(crosses, pl.semaphore_wait, ready_halo, 1)
    pl.when(sp < nz * plane - 1)(halo.start)

    l_hg.wait()
    hg_ref[...] = jax.nn.sigmoid(dot(h_ref[...], whg[...]).astype(BF16).astype(F32))
    l_sg.wait()
    sg_ref[...] = jax.nn.sigmoid(dot(h_ref[...], wsg[...]).astype(BF16).astype(F32))

    cmat[...] = jnp.zeros_like(cmat)
    mmat[...] = jnp.zeros_like(mmat)
    for i in range(PAIRS):
        first = (i % 8) * 32
        value = [jnp.concatenate([t[2 * i], t[2 * i + 1]], axis=1) for t in (out_re, out_im)]
        value[1] = -value[1]
        for part in (0, 1):
            cols = slice(part * 128, part * 128 + 128)
            upper, lower = jnp.where(low, value[part], 0.0), jnp.where(low, 0.0, value[part])
            c_ref[i * 32 : i * 32 + 16, cols] = upper
            c_ref[i * 32 + 16 : i * 32 + 32, cols] = lower
            cols = slice(i * 256 + part * 128, i * 256 + part * 128 + 128)
            cmat[first : first + 16, cols] = upper.astype(BF16)
            cmat[first + 16 : first + 32, cols] = lower.astype(BF16)
    channel = lax.broadcasted_iota(jnp.int32, (2 * PAIRS, 512), 1)
    group = lax.broadcasted_iota(jnp.int32, (2 * PAIRS, 512), 0)
    spread = (channel // 16 == group).astype(F32).astype(BF16)
    rest = skip_t[...]
    spread_skip = jnp.zeros((16, 512), F32)
    for _ in range(3):
        part = rest.astype(BF16)
        spread_skip = spread_skip + dot(part, spread)
        rest = rest - part.astype(F32)
    skip = jnp.sum(
        jnp.where((channel % 16 == group)[:16], spread_skip, 0.0), axis=0, keepdims=True
    )
    for half in (0, 1):
        for k in range(8):
            i = 8 * half + k
            narrow = slice(i * 128, i * 128 + 128)
            summed = dot(tri[0:TOK, :], w_ref[:, i * 256 : i * 256 + 256])
            state = tuple(
                summed[:, 128 * part : 128 * part + 128].reshape(CHUNKS, SEG, 128)
                + entry[i * 16 : i * 16 + 16, :][:, None, :]
                for part, entry in ((0, ent_re), (1, ent_im))
            )
            state = cmul(state, (grow[0, :, narrow][None], grow[1, :, narrow][None]))
            s_ref[:, k * 256 : k * 256 + 128] = state[0].reshape(TOK, 128).astype(BF16)
            s_ref[:, k * 256 + 128 : k * 256 + 256] = state[1].reshape(TOK, 128).astype(BF16)
        cols = slice(half * 256, half * 256 + 256)
        rec = dot_nt(s_ref[...], cmat[:, half * 2048 : half * 2048 + 2048])
        yl_ref[:, cols] = rec * jnp.exp(es_ref[:, cols]) + skip[:, cols] * u_ref[:, cols]

    for k in range(plane):
        when(m != k, plane_wait, s_buf, s_send, s_recv, k)
        when(m != k, plane_wait, l_buf, l_send, l_recv, k)
    state, through = (flat_zero, flat_zero), (flat_one, flat_zero)
    before, before_through = state, through
    plane_shift = flat_zero
    for k in range(plane):
        here = m == k
        before = tuple(jnp.where(here, new, old) for new, old in zip(state, before))
        before_through = tuple(
            jnp.where(here, new, old) for new, old in zip(through, before_through)
        )
        e = jnp.exp(s_buf[k])
        factor = (a_dev[0] * e, a_dev[1] * e)
        through = cmul(factor, through)
        state = cmul(factor, state)
        state = (state[0] + l_buf[k, 0].astype(F32), state[1] + l_buf[k, 1].astype(F32))
        plane_shift = plane_shift + s_buf[k]
    zs_buf[z] = plane_shift
    zl_buf[z, 0] = state[0].astype(BF16)
    zl_buf[z, 1] = state[1].astype(BF16)
    when(z < nz - 1, pl.semaphore_wait, ready_z, nz - 1 - z)

    def z_copy(buf, send, recv, k):
        return remote(buf.at[z], buf.at[z], send.at[k], recv.at[z], (k * plane + m, tp))

    def z_wait(buf, send, recv, k):
        remote(buf.at[k], buf.at[k], send.at[k], recv.at[k], (k * plane + m, tp)).wait_recv()

    for k in range(nz - 1, 0, -1):
        when(z < k, z_copy(zl_buf, zl_send, zl_recv, k).start)
        when(z < k, z_copy(zs_buf, zs_send, zs_recv, k).start)

    seg_power = (flat_one, flat_zero)
    for c in range(CHUNKS):
        at = pl.ds(c, PAIRS, stride=CHUNKS)
        pow_re[at, :] = seg_power[0]
        pow_im[at, :] = seg_power[1]
        seg_power = cmul(seg_power, a_seg)
    for i in range(PAIRS):
        narrow = slice(i * 128, i * 128 + 128)
        start = (pow_re[i * 16 : i * 16 + 16, :][:, None, :], pow_im[i * 16 : i * 16 + 16, :][:, None, :])
        value = cmul(start, (grow[0, :, narrow][None], grow[1, :, narrow][None]))
        for part in (0, 1):
            cols = slice(i * 256 + part * 128, i * 256 + part * 128 + 128)
            g_ref[:, cols] = value[part].reshape(TOK, 128).astype(BF16)
    ed_ref[...] = jnp.exp(shift_sums((col <= row).astype(F32).astype(BF16)))

    @pl.when(sp == 0)
    def _():
        kv_ref[0:WINDOW, :] = jnp.zeros((WINDOW, 512), BF16)

    pl.when(sp > 0)(halo.wait_recv)
    qi = lax.rem(lax.broadcasted_iota(jnp.int32, (2 * WINDOW, 2 * WINDOW), 0), WINDOW)
    key_at = lax.broadcasted_iota(jnp.int32, (2 * WINDOW, 2 * WINDOW), 1)
    inside = (key_at > qi) & (key_at <= qi + WINDOW)
    left = lax.broadcasted_iota(jnp.int32, (WINDOW, 128), 1) < 64
    for n in range(TOK // WINDOW):
        allowed = inside & ((key_at >= WINDOW) | (sp > 0)) if n == 0 else inside
        rows = slice(n * WINDOW, (n + 1) * WINDOW)
        keys = slice(n * WINDOW, (n + 2) * WINDOW)
        for h in range(KV_HEADS):
            q = q_ref[rows, h * 128 : h * 128 + 128]
            turned = pltpu.roll(q, 64, 1)
            in_half = left if h % 2 == 0 else jnp.logical_not(left)
            first, second = (q, turned) if h % 2 == 0 else (turned, q)
            stacked = jnp.concatenate(
                [jnp.where(in_half, part, 0.0).astype(BF16) for part in (first, second)], axis=0
            )
            tile = slice((h // 2) * 128, (h // 2) * 128 + 128)
            scores = dot_nt(stacked, kv_ref[keys, tile])
            scores = jnp.where(allowed, scores, -1e30)
            first_row = lax.broadcasted_iota(jnp.int32, (2 * WINDOW, 1), 0) < WINDOW
            sink_col = jnp.where(first_row, sink[2 * h], sink[2 * h + 1])
            peak = jnp.maximum(jnp.max(scores, axis=1, keepdims=True), sink_col)
            e = jnp.exp(scores - peak)
            total = jnp.sum(e, axis=1, keepdims=True) + jnp.exp(sink_col - peak)
            vtile = slice(256 + (h // 2) * 128, 256 + (h // 2) * 128 + 128)
            mixed = dot(e.astype(BF16), kv_ref[keys, vtile]) / total
            a, b = mixed[:WINDOW], mixed[WINDOW:]
            if h % 2 == 0:
                joined = jnp.where(left, a, pltpu.roll(b, 64, 1))
            else:
                joined = jnp.where(left, pltpu.roll(a, 64, 1), b)
            gate = hg_ref[rows, h * 128 : h * 128 + 128]
            hm_ref[rows, h * 128 : h * 128 + 128] = (gate * joined).astype(BF16)
    l_ho.wait()
    acc_ref[...] = dot(hm_ref[...], who[...])

    pre[...] = jnp.zeros_like(pre)
    for k in range(nz - 1):

        @pl.when(k < z)
        def _(k=k):
            z_wait(zs_buf, zs_send, zs_recv, k)
            z_wait(zl_buf, zl_send, zl_recv, k)
            e = jnp.exp(zs_buf[k])
            new = cmul((a_plane[0] * e, a_plane[1] * e), (pre[0], pre[1]))
            pre[0] = new[0] + zl_buf[k, 0].astype(F32)
            pre[1] = new[1] + zl_buf[k, 1].astype(F32)

    carry = cmul(before_through, (pre[0], pre[1]))
    carry = (before[0] + carry[0], before[1] + carry[1])
    for i in range(PAIRS):
        first = (i % 8) * 32
        value = (c_ref[i * 32 : i * 32 + 32, 0:128], c_ref[i * 32 : i * 32 + 32, 128:256])
        value = cmul(value, (carry[0][i : i + 1, :], -carry[1][i : i + 1, :]))
        for part in (0, 1):
            cols = slice(i * 256 + part * 128, i * 256 + part * 128 + 128)
            mmat[first : first + 32, cols] = value[part].astype(BF16)
    for half in (0, 1):
        cols = slice(half * 256, half * 256 + 256)
        wide = slice(half * 2048, half * 2048 + 2048)
        rec = dot_nt(g_ref[:, wide], mmat[:, wide])
        rec = rec * ed_ref[:, cols] + yl_ref[:, cols]
        sm_ref[:, cols] = (sg_ref[:, cols] * jax.nn.gelu(rec)).astype(BF16)

    l_so.wait()
    outs = []
    for k in range(N_OUT):
        cols = pl.ds(pl.multiple_of(other * HALF + k * 256, 256), 256)
        psend[k] = (acc_ref[:, cols] + dot(sm_ref[...], wso[:, cols])).astype(BF16)
        copy = remote(psend.at[k], precv.at[k], out_send.at[k], out_recv.at[k], (sp, other))
        copy.start()
        outs.append(copy)
    for k in range(N_OUT):
        cols = pl.ds(pl.multiple_of(tp * HALF + k * 256, 256), 256)
        own = acc_ref[:, cols] + dot(sm_ref[...], wso[:, cols])
        outs[k].wait_recv()
        out[:, k * 256 : k * 256 + 256] = (own + precv[k].astype(F32)).astype(BF16)

    send_h.wait_send()
    pl.when(sp < nz * plane - 1)(halo.wait_send)
    for copy in outs:
        copy.wait_send()
    for k in range(plane):
        when(m != k, plane_copy(s_buf, s_send, s_recv, k).wait_send)
        when(m != k, plane_copy(l_buf, l_send, l_recv, k).wait_send)
    for k in range(1, nz):
        when(z < k, z_copy(zs_buf, zs_send, zs_recv, k).wait_send)
        when(z < k, z_copy(zl_buf, zl_send, zl_recv, k).wait_send)


def on_device(
    sizes,
    hidden,
    query_weight,
    key_weight,
    value_weight,
    head_gate_weight,
    state_in_weight,
    state_gate_weight,
    sink_logit,
    decay_real,
    decay_frequency,
    log_step,
    input_real,
    input_imaginary,
    output_real,
    output_imaginary,
    skip_weight,
    decay_shift,
    head_out_weight,
    state_out_weight,
):
    nz, ny, nx = sizes
    vmem = pl.BlockSpec(memory_space=pltpu.VMEM)
    hbm = pl.BlockSpec(memory_space=pl.ANY)
    plane = ny * nx
    scratch = [
        ((2 * PAIRS, 64), F32),
        ((2 * PAIRS, 64), F32),
        ((2 * PAIRS, 16, 64), F32),
        ((2 * PAIRS, 16, 64), F32),
        ((2 * PAIRS, 16, 64), F32),
        ((2 * PAIRS, 16, 64), F32),
        ((16, 2 * PAIRS), F32),
        ((2 * PAIRS, TOK), F32),
        ((TOK, D), BF16),
        ((D, 512), BF16),
        ((D, 512), BF16),
        ((D, 512), BF16),
        ((D, 512), BF16),
        ((D, 512), BF16),
        ((512, D), BF16),
        ((512, D), BF16),
        ((128, LANES), BF16),
        ((256, LANES), BF16),
        ((256, LANES), BF16),
        ((512, 256), F32),
        ((TOK + CHUNKS, TOK), BF16),
        ((2, SEG, PAIRS * 128), F32),
        ((2, SEG, PAIRS * 128), F32),
        ((CHUNKS, PAIRS, 128), F32),
        ((2 * PAIRS, 128), F32),
        ((TOK, 512), F32),
        ((TOK, 512), BF16),
        ((TOK, 512), F32),
        ((TOK, 512), F32),
        ((TOK, LANES), BF16),
        ((TOK, LANES // 2), BF16),
        ((TOK, LANES), BF16),
        ((TOK, 512), F32),
        ((PAIRS * CHUNKS, 128), F32),
        ((PAIRS * CHUNKS, 128), F32),
        ((PAIRS * CHUNKS, 128), F32),
        ((PAIRS * CHUNKS, 128), F32),
        ((PAIRS * CHUNKS, 128), F32),
        ((PAIRS * CHUNKS, 128), F32),
        ((TOK, 512), F32),
        ((TOK + WINDOW, 512), BF16),
        ((TOK, 512), F32),
        ((TOK, 512), F32),
        ((TOK, 512), BF16),
        ((TOK, 512), BF16),
        ((TOK, D), F32),
        ((N_OUT, TOK, 256), BF16),
        ((N_OUT, TOK, 256), BF16),
        ((plane, PAIRS, 128), F32),
        ((plane, 2, PAIRS, 128), BF16),
        ((nz, PAIRS, 128), F32),
        ((nz, 2, PAIRS, 128), BF16),
        ((2, PAIRS, 128), F32),
    ]
    dma = pltpu.SemaphoreType.DMA
    regular = pltpu.SemaphoreType.REGULAR
    return pl.pallas_call(
        functools.partial(kernel, sizes),
        out_shape=jax.ShapeDtypeStruct((TOK, HALF), BF16),
        in_specs=[hbm] * 19,
        out_specs=vmem,
        scratch_shapes=[pltpu.SMEM((8,), F32), pltpu.SMEM((2 * PAIRS,), F32)]
        + [pltpu.VMEM(shape, dtype) for shape, dtype in scratch]
        + [dma((19,)), dma((2,)), dma((2,)), dma((N_OUT,)), dma((N_OUT,))]
        + [dma((plane,))] * 4
        + [dma((nz,))] * 4
        + [regular] * 3,
        compiler_params=pltpu.CompilerParams(
            collective_id=0, has_side_effects=True, vmem_limit_bytes=60 * 1024 * 1024
        ),
        name="layer",
    )(
        hidden,
        query_weight,
        key_weight,
        value_weight,
        head_gate_weight,
        state_in_weight,
        state_gate_weight,
        head_out_weight,
        state_out_weight,
        sink_logit,
        log_step,
        decay_real,
        decay_frequency,
        input_real.transpose(0, 2, 1),
        input_imaginary.transpose(0, 2, 1),
        output_real,
        output_imaginary,
        skip_weight.T,
        decay_shift,
    )


def solution(mesh):
    sizes = SP_SIZES[mesh.shape["sp"]]
    in_specs = (
        P("sp", "tp"),
        P(None, "tp"),
        P(None, "tp"),
        P(None, "tp"),
        P(None, "tp"),
        P(None, "tp"),
        P(None, "tp"),
        P("tp"),
        P("tp", None),
        P("tp", None),
        P("tp"),
        P("tp", None, None),
        P("tp", None, None),
        P("tp", None, None),
        P("tp", None, None),
        P("tp", None),
        P("tp", "sp"),
        P("tp", None),
        P("tp", None),
    )
    return jax.shard_map(
        functools.partial(on_device, sizes),
        mesh=mesh,
        in_specs=in_specs,
        out_specs=P("sp", "tp"),
        check_vma=False,
    )
```

```python
import functools

import jax
import jax.numpy as jnp
from jax import lax
from jax.experimental import pallas as pl
from jax.experimental.pallas import tpu as pltpu
from jax.sharding import PartitionSpec as P

MESH = pl.DeviceIdType.MESH
F32 = jnp.float32
BF16 = jnp.bfloat16

TOK = 256
D = 2048
HALF = D // 2
WINDOW = 128
SEG = 16
CHUNKS = TOK // SEG
PAIRS = 16
LANES = PAIRS * 256
KV_HEADS = 4
SP_SIZES = {128: (8, 4, 4), 8: (2, 2, 2)}

FAR = 3
N_OUT = 2


def dot(a, b):
    return jnp.dot(a, b, preferred_element_type=F32)


def dot_nt(a, b):
    return lax.dot_general(a, b, (((1,), (1,)), ((), ())), preferred_element_type=F32)


def cmul(a, b):
    return (a[0] * b[0] - a[1] * b[1], a[0] * b[1] + a[1] * b[0])


def csquares(a, times):
    for _ in range(times):
        a = cmul(a, a)
    return a


def log2(n):
    return n.bit_length() - 1


def kernel(sizes, *refs):
    nz, ny, nx = sizes
    plane = ny * nx
    (
        hidden,
        w_query,
        w_key,
        w_value,
        w_hgate,
        w_sin,
        w_sgate,
        w_hout,
        w_sout,
        sink_in,
        step_in,
        real_in,
        freq_in,
        in_re_in,
        in_im_in,
        out_re_in,
        out_im_in,
        skip_in,
        shift_in,
        out,
        sink,
        log_step,
        decay_real,
        decay_freq,
        in_re,
        in_im,
        out_re,
        out_im,
        skip_t,
        shift,
        h_ref,
        win,
        wkvq,
        wgate,
        who,
        wso,
        drive,
        cmat,
        skip_ref,
        bias,
        tri,
        grow,
        shrink,
        decay,
        pair_tile,
        u_ref,
        us_ref,
        es_ref,
        x_ref,
        s_ref,
        tot_re,
        tot_im,
        ent_re,
        ent_im,
        q_ref,
        kv_ref,
        hg_ref,
        sg_ref,
        hm_ref,
        sm_ref,
        acc_ref,
        psend,
        precv,
        s_buf,
        l_buf,
        zs_buf,
        zl_buf,
        pre,
        load_sem,
        h_sem,
        halo_sem,
        out_send,
        out_recv,
        s_send,
        s_recv,
        l_send,
        l_recv,
        zs_send,
        zs_recv,
        zl_send,
        zl_recv,
        ready_near,
        ready_far,
        ready_z,
    ) = refs
    sp, tp = lax.axis_index("sp"), lax.axis_index("tp")
    z, m = sp // plane, sp % plane
    other = 1 - tp

    apart = [k % nx + k // nx - (m % nx + m // nx) for k in range(plane)]
    behind = [
        jnp.logical_or(apart[k] > 0, jnp.logical_and(apart[k] == 0, k > m)) for k in range(plane)
    ]
    ahead = [
        jnp.logical_or(apart[k] < 0, jnp.logical_and(apart[k] == 0, k < m)) for k in range(plane)
    ]

    def count(conditions):
        return sum(condition.astype(jnp.int32) for condition in conditions)

    barrier = pltpu.get_barrier_semaphore()

    def signal(semaphore, device):
        pl.semaphore_signal(semaphore, inc=1, device_id=device, device_id_type=MESH)

    def when(condition, act, *args):
        pl.when(condition)(functools.partial(act, *args))

    crosses = jnp.logical_and(m == plane - 1, z < nz - 1)
    crossed = jnp.logical_and(m == 0, z > 0)
    signal(barrier, (sp, other))
    for k in range(plane):
        when(behind[k], signal, barrier, (z * plane + k, tp))
    for r in range(1, nz):
        when(z + r < nz, signal, barrier, (sp + r * plane, tp))
    when(crossed, signal, barrier, (sp - 1, tp))
    loads = []

    def load(src, dst):
        copy = pltpu.make_async_copy(src, dst, load_sem.at[len(loads)])
        copy.start()
        loads.append(copy)
        return copy

    def remote(src, dst, send, recv, device):
        return pltpu.make_async_remote_copy(
            src_ref=src,
            dst_ref=dst,
            send_sem=send,
            recv_sem=recv,
            device_id=device,
            device_id_type=MESH,
        )

    mine = pl.ds(pl.multiple_of(tp * HALF, HALF), HALF)
    theirs = pl.ds(pl.multiple_of(other * HALF, HALF), HALF)
    l_h = load(hidden, h_ref.at[:, mine])
    small = [
        load(src, dst)
        for src, dst in (
            (step_in, log_step),
            (real_in, decay_real),
            (freq_in, decay_freq),
            (shift_in, shift),
            (in_re_in, in_re),
            (in_im_in, in_im),
            (out_re_in, out_re),
            (out_im_in, out_im),
            (skip_in, skip_t),
            (sink_in, sink),
        )
    ]
    l_in = load(w_sin, win)

    pl.semaphore_wait(barrier, 1 + count(ahead) + z + count([crosses]))
    l_h.wait()
    send_h = remote(h_ref.at[:, mine], h_ref.at[:, mine], h_sem.at[0], h_sem.at[1], (sp, other))
    send_h.start()
    for k in range(plane):
        far = apart[k] <= -FAR
        when(far, signal, ready_far, (z * plane + k, tp))
        close = jnp.logical_and(ahead[k], jnp.logical_not(far))
        when(close, signal, ready_near, (z * plane + k, tp))
    for r in range(1, nz):
        when(z >= r, signal, ready_z, (sp - r * plane, tp))
    l_k = load(w_key, wkvq.at[:, 0:256])
    l_v = load(w_value, wkvq.at[:, 256:512])
    l_q = load(w_query, wkvq.at[:, 512:1024])

    for copy in small:
        copy.wait()
    low = lax.broadcasted_iota(jnp.int32, (PAIRS, 128), 1) < 64

    def paired(value):
        pair_tile[...] = jnp.concatenate([value, value], axis=1)
        even = pair_tile[pl.ds(0, PAIRS, stride=2), :]
        odd = pair_tile[pl.ds(1, PAIRS, stride=2), :]
        return jnp.where(low, even, odd)

    pair_row = lax.broadcasted_iota(jnp.int32, (PAIRS, 128), 0)
    step = jnp.zeros((PAIRS, 128), F32)
    for i in range(PAIRS):
        step = jnp.where(
            pair_row == i, jnp.where(low, log_step[2 * i], log_step[2 * i + 1]), step
        )
    step = jnp.exp(step)
    real, freq = paired(decay_real[...]), paired(decay_freq[...])
    magnitude, inverse = jnp.exp(real * step), jnp.exp(-(real * step))
    cosine, sine = jnp.cos(freq * step), jnp.sin(freq * step)
    base = (magnitude * cosine, magnitude * sine)
    base_inv = (inverse * cosine, -(inverse * sine))
    denominator = real * real + freq * freq
    less = base[0] - 1.0
    zoh = (
        (less * real + base[1] * freq) / denominator,
        (base[1] * real - less * freq) / denominator,
    )

    row = lax.broadcasted_iota(jnp.int32, (TOK, TOK), 0)
    col = lax.broadcasted_iota(jnp.int32, (TOK, TOK), 1)
    tri[0:TOK, :] = ((row // SEG == col // SEG) & (col <= row)).astype(F32).astype(BF16)
    srow = lax.broadcasted_iota(jnp.int32, (CHUNKS, TOK), 0)
    scol = lax.broadcasted_iota(jnp.int32, (CHUNKS, TOK), 1)
    tri[TOK:, :] = (scol // SEG == srow).astype(F32).astype(BF16)
    drive[...] = jnp.zeros_like(drive)
    for i in range(PAIRS):
        factor = (zoh[0][i : i + 1, :], zoh[1][i : i + 1, :])
        first = (i % 4) * 32
        value = cmul(factor, tuple(jnp.concatenate([t[2 * i], t[2 * i + 1]], axis=1) for t in (in_re, in_im)))
        for part in (0, 1):
            cols = slice(i * 256 + part * 128, i * 256 + part * 128 + 128)
            drive[first : first + 16, cols] = jnp.where(low, value[part], 0.0).astype(BF16)
            drive[first + 16 : first + 32, cols] = jnp.where(low, 0.0, value[part]).astype(BF16)

    cmat[...] = jnp.zeros_like(cmat)
    for i in range(PAIRS):
        first = (i % 8) * 32
        value = [jnp.concatenate([t[2 * i], t[2 * i + 1]], axis=1) for t in (out_re, out_im)]
        value[1] = -value[1]
        for part in (0, 1):
            cols = slice(i * 256 + part * 128, i * 256 + part * 128 + 128)
            cmat[first : first + 16, cols] = jnp.where(low, value[part], 0.0).astype(BF16)
            cmat[first + 16 : first + 32, cols] = jnp.where(low, 0.0, value[part]).astype(BF16)
    channel = lax.broadcasted_iota(jnp.int32, (2 * PAIRS, 512), 1)
    group = lax.broadcasted_iota(jnp.int32, (2 * PAIRS, 512), 0)
    spread = (channel // 16 == group).astype(F32).astype(BF16)
    rest = skip_t[...]
    spread_skip = jnp.zeros((16, 512), F32)
    for _ in range(3):
        part = rest.astype(BF16)
        spread_skip = spread_skip + dot(part, spread)
        rest = rest - part.astype(F32)
    skip_ref[...] = jnp.sum(
        jnp.where((channel % 16 == group)[:16], spread_skip, 0.0), axis=0, keepdims=True
    )
    qi = lax.rem(row, WINDOW)
    inside = (col > qi) & (col <= qi + WINDOW)
    bias[0] = jnp.where(inside & ((col >= WINDOW) | (sp > 0)), 0.0, -1e30)
    bias[1] = jnp.where(inside, 0.0, -1e30)

    power = lax.broadcasted_iota(jnp.int32, (8, 128), 0) + 1
    ones, zeros = jnp.ones((8, 128), F32), jnp.zeros((8, 128), F32)
    for table, root in ((grow, base), (shrink, base_inv)):
        for i in range(PAIRS):
            b = tuple(jnp.broadcast_to(part[i : i + 1, :], (8, 128)) for part in root)
            value = (ones, zeros)
            for bit in range(4):
                has = (power >> bit) & 1 == 1
                value = cmul(value, (jnp.where(has, b[0], ones), jnp.where(has, b[1], zeros)))
                if bit < 3:
                    b = cmul(b, b)
            cols = slice(i * 128, i * 128 + 128)
            upper = cmul(value, b)
            for k in (0, 1):
                table[k, 0:8, cols] = value[k]
                table[k, 8:16, cols] = upper[k]
    a_seg = csquares(base, log2(SEG))
    a_dev = csquares(a_seg, log2(CHUNKS))
    a_plane = csquares(a_dev, log2(plane))

    def shift_sums(mask):
        rest = jnp.broadcast_to(shift[...][:, None, :], (2 * PAIRS, 16, TOK)).reshape(512, TOK)
        sums = None
        for _ in range(3):
            part = rest.astype(BF16)
            term = dot_nt(mask, part)
            sums = term if sums is None else sums + term
            rest = rest - part.astype(F32)
        return sums

    es_ref[...] = shift_sums(tri[0:TOK, :])
    lane = lax.broadcasted_iota(jnp.int32, (PAIRS, 128), 1)
    total_shift = jnp.zeros((PAIRS, 128), F32)
    for c in range(CHUNKS):
        if c % 8 == 0:
            pair_tile[...] = shift[:, c * SEG : c * SEG + 128]
            even = pair_tile[pl.ds(0, PAIRS, stride=2), :]
            odd = pair_tile[pl.ds(1, PAIRS, stride=2), :]
        inside = lane // SEG == c % 8
        s = jnp.where(
            low,
            jnp.sum(jnp.where(inside, even, 0.0), axis=1, keepdims=True),
            jnp.sum(jnp.where(inside, odd, 0.0), axis=1, keepdims=True),
        )
        total_shift = total_shift + s
        decay[c] = jnp.exp(s)
    s_buf[m] = jnp.sum(
        jnp.where(lane % 64 == pair_row, total_shift, 0.0), axis=0, keepdims=True
    )

    l_in.wait()
    u_ref[...] = dot(h_ref[:, mine], win[mine, :])
    send_h.wait_recv()
    l_hg = load(w_hgate, wgate.at[:, 0:512])
    l_sg = load(w_sgate, wgate.at[:, 512:1024])
    l_ho = load(w_hout, who)
    l_so = load(w_sout, wso)
    row_end = m % nx == nx - 1
    l_k.wait()
    l_v.wait()
    halo = remote(
        kv_ref.at[TOK : TOK + WINDOW, :],
        kv_ref.at[0:WINDOW, :],
        halo_sem.at[0],
        halo_sem.at[1],
        (lax.rem(sp + 1, nz * plane), tp),
    )

    @pl.when(row_end)
    def _():
        kv_ref[TOK:, :] = dot(h_ref[WINDOW:, :], wkvq[:, 0:512]).astype(BF16)

    u = (u_ref[...] + dot(h_ref[:, theirs], win[theirs, :])).astype(BF16).astype(F32)
    u_ref[...] = u
    us_ref[...] = (u * jnp.exp(-es_ref[...])).astype(BF16)
    pl.when(jnp.logical_and(row_end, sp < nz * plane - 1))(halo.start)

    def plane_copy(buf, send, recv, k):
        return remote(buf.at[m], buf.at[m], send.at[k], recv.at[m], (z * plane + k, tp))

    def plane_wait(buf, send, recv, k):
        remote(buf.at[k], buf.at[k], send.at[k], recv.at[k], (z * plane + k, tp)).wait_recv()

    for i in range(PAIRS):
        cols, narrow = slice(i * 256, i * 256 + 256), slice(i * 128, i * 128 + 128)
        j = i // 4
        push = dot(us_ref[:, j * 128 : j * 128 + 128], drive[:, cols])
        push = (push[:, :128].reshape(CHUNKS, SEG, 128), push[:, 128:].reshape(CHUNKS, SEG, 128))
        back = (shrink[0, :, narrow][None], shrink[1, :, narrow][None])
        w = cmul(push, back)
        w = jnp.concatenate([part.reshape(TOK, 128).astype(BF16) for part in w], axis=1)
        summed = dot(tri[...], w)
        x_ref[:, cols] = summed[:TOK]
        tot_re[i * 16 : i * 16 + 16, :] = summed[TOK:, :128]
        tot_im[i * 16 : i * 16 + 16, :] = summed[TOK:, 128:]

    flat_zero = jnp.zeros((PAIRS, 128), F32)
    flat_one = jnp.ones((PAIRS, 128), F32)

    def chunk_scan(state, keep):
        for c in range(CHUNKS):
            at = pl.ds(c, PAIRS, stride=CHUNKS)
            if keep:
                ent_re[at, :] = state[0]
                ent_im[at, :] = state[1]
            e = decay[c]
            state = cmul(
                (state[0] + tot_re[at, :], state[1] + tot_im[at, :]), (a_seg[0] * e, a_seg[1] * e)
            )
        return state

    state = chunk_scan((flat_zero, flat_zero), False)
    l_buf[m, 0] = state[0].astype(BF16)
    l_buf[m, 1] = state[1].astype(BF16)
    def send_to(k, condition):
        when(condition, plane_copy(l_buf, l_send, l_recv, k).start)
        when(condition, plane_copy(s_buf, s_send, s_recv, k).start)

    near = [jnp.logical_and(behind[k], apart[k] < FAR) for k in range(plane)]
    far = [apart[k] >= FAR for k in range(plane)]
    for k in range(plane):
        send_to(k, ahead[k])
    when(count(near) > 0, pl.semaphore_wait, ready_near, jnp.maximum(count(near), 1))
    for k in range(plane):
        send_to(k, near[k])

    l_q.wait()
    rows = dot(h_ref[...], wkvq[...]).astype(BF16)
    kv_ref[WINDOW:TOK, :] = rows[0:WINDOW, 0:512]
    q_ref[...] = rows[:, 512:1024].astype(F32) * 0.125

    @pl.when(jnp.logical_not(row_end))
    def _():
        kv_ref[TOK:, :] = rows[WINDOW:, 0:512]

    pl.when(jnp.logical_not(row_end))(halo.start)
    when(count(far) > 0, pl.semaphore_wait, ready_far, jnp.maximum(count(far), 1))
    for k in range(plane):
        send_to(k, far[k])

    l_hg.wait()
    l_sg.wait()
    gates = jax.nn.sigmoid(dot(h_ref[...], wgate[...]).astype(BF16).astype(F32))
    hg_ref[...] = gates[:, 0:512]
    sg_ref[...] = gates[:, 512:1024]

    left = lax.broadcasted_iota(jnp.int32, (WINDOW, 128), 1) < 64

    def attend(n):
        rows = slice(n * WINDOW, (n + 1) * WINDOW)
        keys = slice(n * WINDOW, (n + 2) * WINDOW)
        for h in range(KV_HEADS):
            q = q_ref[rows, h * 128 : h * 128 + 128]
            turned = pltpu.roll(q, 64, 1)
            in_half = left if h % 2 == 0 else jnp.logical_not(left)
            first, second = (q, turned) if h % 2 == 0 else (turned, q)
            stacked = jnp.concatenate(
                [jnp.where(in_half, part, 0.0).astype(BF16) for part in (first, second)], axis=0
            )
            tile = slice((h // 2) * 128, (h // 2) * 128 + 128)
            scores = dot_nt(stacked, kv_ref[keys, tile]) + bias[n]
            first_row = lax.broadcasted_iota(jnp.int32, (2 * WINDOW, 1), 0) < WINDOW
            sink_col = jnp.where(first_row, sink[2 * h], sink[2 * h + 1])
            peak = jnp.maximum(jnp.max(scores, axis=1, keepdims=True), sink_col)
            e = jnp.exp(scores - peak)
            total = jnp.sum(e, axis=1, keepdims=True) + jnp.exp(sink_col - peak)
            vtile = slice(256 + (h // 2) * 128, 256 + (h // 2) * 128 + 128)
            mixed = dot(e.astype(BF16), kv_ref[keys, vtile]) / total
            a, b = mixed[:WINDOW], mixed[WINDOW:]
            if h % 2 == 0:
                joined = jnp.where(left, a, pltpu.roll(b, 64, 1))
            else:
                joined = jnp.where(left, pltpu.roll(a, 64, 1), b)
            gate = hg_ref[rows, h * 128 : h * 128 + 128]
            hm_ref[rows, h * 128 : h * 128 + 128] = (gate * joined).astype(BF16)
    attend(1)

    for k in range(plane):
        when(m != k, plane_wait, s_buf, s_send, s_recv, k)
        when(m != k, plane_wait, l_buf, l_send, l_recv, k)
    state, through = (flat_zero, flat_zero), (flat_one, flat_zero)
    before, before_through = state, through
    plane_shift = jnp.zeros((1, 128), F32)

    def spread_row(sums):
        own = jnp.where(lane % 64 == pair_row, sums, 0.0)
        return jnp.where(
            low,
            jnp.sum(jnp.where(low, own, 0.0), axis=1, keepdims=True),
            jnp.sum(jnp.where(low, 0.0, own), axis=1, keepdims=True),
        )

    for k in range(plane):
        here = m == k
        before = tuple(jnp.where(here, new, old) for new, old in zip(state, before))
        before_through = tuple(
            jnp.where(here, new, old) for new, old in zip(through, before_through)
        )
        e = jnp.exp(spread_row(s_buf[k]))
        factor = (a_dev[0] * e, a_dev[1] * e)
        through = cmul(factor, through)
        state = cmul(factor, state)
        state = (state[0] + l_buf[k, 0].astype(F32), state[1] + l_buf[k, 1].astype(F32))
        plane_shift = plane_shift + s_buf[k]
    zs_buf[z] = plane_shift
    zl_buf[z, 0] = state[0].astype(BF16)
    zl_buf[z, 1] = state[1].astype(BF16)
    when(z < nz - 1, pl.semaphore_wait, ready_z, nz - 1 - z)

    def z_copy(buf, send, recv, k):
        return remote(buf.at[z], buf.at[z], send.at[k], recv.at[z], (k * plane + m, tp))

    def z_wait(buf, send, recv, k):
        remote(buf.at[k], buf.at[k], send.at[k], recv.at[k], (k * plane + m, tp)).wait_recv()

    for k in range(nz - 1, 0, -1):
        when(z < k, z_copy(zl_buf, zl_send, zl_recv, k).start)
        when(z < k, z_copy(zs_buf, zs_send, zs_recv, k).start)

    l_ho.wait()

    @pl.when(sp == 0)
    def _():
        kv_ref[0:WINDOW, :] = jnp.zeros((WINDOW, 512), BF16)

    pl.when(sp > 0)(halo.wait_recv)
    attend(0)
    acc_ref[...] = dot(hm_ref[...], who[...])

    pre[...] = jnp.zeros_like(pre)
    for k in range(nz - 1):

        @pl.when(k < z)
        def _(k=k):
            z_wait(zs_buf, zs_send, zs_recv, k)
            z_wait(zl_buf, zl_send, zl_recv, k)
            e = jnp.exp(spread_row(zs_buf[k]))
            new = cmul((a_plane[0] * e, a_plane[1] * e), (pre[0], pre[1]))
            pre[0] = new[0] + zl_buf[k, 0].astype(F32)
            pre[1] = new[1] + zl_buf[k, 1].astype(F32)

    carry = cmul(before_through, (pre[0], pre[1]))
    carry = (before[0] + carry[0], before[1] + carry[1])
    chunk_scan(carry, True)
    for half in (0, 1):
        for k in range(8):
            i = 8 * half + k
            narrow = slice(i * 128, i * 128 + 128)
            growth = (grow[0, :, narrow], grow[1, :, narrow])
            for c in range(CHUNKS):
                rows = slice(c * SEG, c * SEG + SEG)
                entry = i * CHUNKS + c
                re, im = slice(i * 256, i * 256 + 128), slice(i * 256 + 128, i * 256 + 256)
                state = (
                    x_ref[rows, re] + ent_re[entry : entry + 1, :],
                    x_ref[rows, im] + ent_im[entry : entry + 1, :],
                )
                state = cmul(state, growth)
                s_ref[rows, re] = state[0].astype(BF16)
                s_ref[rows, im] = state[1].astype(BF16)
        cols = slice(half * 256, half * 256 + 256)
        wide = slice(half * 2048, half * 2048 + 2048)
        rec = dot_nt(s_ref[:, wide], cmat[:, wide])
        rec = rec * jnp.exp(es_ref[:, cols]) + skip_ref[:, cols] * u_ref[:, cols]
        sm_ref[:, cols] = (sg_ref[:, cols] * jax.nn.gelu(rec)).astype(BF16)

    l_so.wait()
    outs = []
    width = HALF // N_OUT
    for k in range(N_OUT):
        cols = pl.ds(pl.multiple_of(other * HALF + k * width, width), width)
        psend[k] = (acc_ref[:, cols] + dot(sm_ref[...], wso[:, cols])).astype(BF16)
        copy = remote(psend.at[k], precv.at[k], out_send.at[k], out_recv.at[k], (sp, other))
        copy.start()
        outs.append(copy)
    acc_ref[:, mine] = acc_ref[:, mine] + dot(sm_ref[...], wso[:, mine])
    for k in range(N_OUT):
        cols = pl.ds(pl.multiple_of(tp * HALF + k * width, width), width)
        outs[k].wait_recv()
        out[:, k * width : k * width + width] = (acc_ref[:, cols] + precv[k].astype(F32)).astype(BF16)

    send_h.wait_send()
    pl.when(sp < nz * plane - 1)(halo.wait_send)
    for copy in outs:
        copy.wait_send()
    for k in range(plane):
        when(m != k, plane_copy(s_buf, s_send, s_recv, k).wait_send)
        when(m != k, plane_copy(l_buf, l_send, l_recv, k).wait_send)
    for k in range(1, nz):
        when(z < k, z_copy(zs_buf, zs_send, zs_recv, k).wait_send)
        when(z < k, z_copy(zl_buf, zl_send, zl_recv, k).wait_send)


def on_device(
    sizes,
    hidden,
    query_weight,
    key_weight,
    value_weight,
    head_gate_weight,
    state_in_weight,
    state_gate_weight,
    sink_logit,
    decay_real,
    decay_frequency,
    log_step,
    input_real,
    input_imaginary,
    output_real,
    output_imaginary,
    skip_weight,
    decay_shift,
    head_out_weight,
    state_out_weight,
):
    nz, ny, nx = sizes
    vmem = pl.BlockSpec(memory_space=pltpu.VMEM)
    hbm = pl.BlockSpec(memory_space=pl.ANY)
    plane = ny * nx
    scratch = [
        ((2 * PAIRS, 64), F32),
        ((2 * PAIRS, 64), F32),
        ((2 * PAIRS, 16, 64), F32),
        ((2 * PAIRS, 16, 64), F32),
        ((2 * PAIRS, 16, 64), F32),
        ((2 * PAIRS, 16, 64), F32),
        ((16, 2 * PAIRS), F32),
        ((2 * PAIRS, TOK), F32),
        ((TOK, D), BF16),
        ((D, 512), BF16),
        ((D, 1024), BF16),
        ((D, 1024), BF16),
        ((512, D), BF16),
        ((512, D), BF16),
        ((128, LANES), BF16),
        ((256, LANES), BF16),
        ((1, 512), F32),
        ((2, TOK, TOK), F32),
        ((TOK + CHUNKS, TOK), BF16),
        ((2, SEG, PAIRS * 128), F32),
        ((2, SEG, PAIRS * 128), F32),
        ((CHUNKS, PAIRS, 128), F32),
        ((2 * PAIRS, 128), F32),
        ((TOK, 512), F32),
        ((TOK, 512), BF16),
        ((TOK, 512), F32),
        ((TOK, LANES), F32),
        ((TOK, LANES), BF16),
        ((PAIRS * CHUNKS, 128), F32),
        ((PAIRS * CHUNKS, 128), F32),
        ((PAIRS * CHUNKS, 128), F32),
        ((PAIRS * CHUNKS, 128), F32),
        ((TOK, 512), F32),
        ((TOK + WINDOW, 512), BF16),
        ((TOK, 512), F32),
        ((TOK, 512), F32),
        ((TOK, 512), BF16),
        ((TOK, 512), BF16),
        ((TOK, D), F32),
        ((N_OUT, TOK, HALF // N_OUT), BF16),
        ((N_OUT, TOK, HALF // N_OUT), BF16),
        ((plane, 1, 128), F32),
        ((plane, 2, PAIRS, 128), BF16),
        ((nz, 1, 128), F32),
        ((nz, 2, PAIRS, 128), BF16),
        ((2, PAIRS, 128), F32),
    ]
    dma = pltpu.SemaphoreType.DMA
    regular = pltpu.SemaphoreType.REGULAR
    return pl.pallas_call(
        functools.partial(kernel, sizes),
        out_shape=jax.ShapeDtypeStruct((TOK, HALF), BF16),
        in_specs=[hbm] * 19,
        out_specs=vmem,
        scratch_shapes=[pltpu.SMEM((8,), F32), pltpu.SMEM((2 * PAIRS,), F32)]
        + [pltpu.VMEM(shape, dtype) for shape, dtype in scratch]
        + [dma((19,)), dma((2,)), dma((2,)), dma((N_OUT,)), dma((N_OUT,))]
        + [dma((plane,))] * 4
        + [dma((nz,))] * 4
        + [regular] * 3,
        compiler_params=pltpu.CompilerParams(
            collective_id=0, has_side_effects=True, vmem_limit_bytes=48 * 1024 * 1024
        ),
        name="layer",
    )(
        *(
            pltpu.with_memory_space_constraint(array, pltpu.HBM)
            for array in (
                hidden,
                query_weight,
                key_weight,
                value_weight,
                head_gate_weight,
                state_in_weight,
                state_gate_weight,
                head_out_weight,
                state_out_weight,
                sink_logit,
                log_step,
                decay_real,
                decay_frequency,
                input_real.transpose(0, 2, 1),
                input_imaginary.transpose(0, 2, 1),
                output_real,
                output_imaginary,
                skip_weight.T,
                decay_shift,
            )
        )
    )


def solution(mesh):
    sizes = SP_SIZES[mesh.shape["sp"]]
    in_specs = (
        P("sp", "tp"),
        P(None, "tp"),
        P(None, "tp"),
        P(None, "tp"),
        P(None, "tp"),
        P(None, "tp"),
        P(None, "tp"),
        P("tp"),
        P("tp", None),
        P("tp", None),
        P("tp"),
        P("tp", None, None),
        P("tp", None, None),
        P("tp", None, None),
        P("tp", None, None),
        P("tp", None),
        P("tp", "sp"),
        P("tp", None),
        P("tp", None),
    )
    return jax.shard_map(
        functools.partial(on_device, sizes),
        mesh=mesh,
        in_specs=in_specs,
        out_specs=P("sp", "tp"),
        check_vma=False,
    )
```

```python
import functools

import jax
import jax.numpy as jnp
from jax import lax
from jax.experimental import pallas as pl
from jax.experimental.pallas import tpu as pltpu
from jax.sharding import PartitionSpec as P

MESH = pl.DeviceIdType.MESH
F32 = jnp.float32
BF16 = jnp.bfloat16

TOK = 256
D = 2048
HALF = D // 2
WINDOW = 128
SEG = 16
CHUNKS = TOK // SEG
PAIRS = 16
LANES = PAIRS * 256
KV_HEADS = 4
SP_SIZES = {128: (8, 4, 4), 8: (2, 2, 2)}

FAR = 3
N_OUT = 2


def dot(a, b):
    return jnp.dot(a, b, preferred_element_type=F32)


def dot_nt(a, b):
    return lax.dot_general(a, b, (((1,), (1,)), ((), ())), preferred_element_type=F32)


def cmul(a, b):
    return (a[0] * b[0] - a[1] * b[1], a[0] * b[1] + a[1] * b[0])


def csquares(a, times):
    for _ in range(times):
        a = cmul(a, a)
    return a


def log2(n):
    return n.bit_length() - 1


def kernel(sizes, *refs):
    nz, ny, nx = sizes
    plane = ny * nx
    (
        hidden,
        w_query,
        w_key,
        w_value,
        w_hgate,
        w_sin,
        w_sgate,
        w_hout,
        w_sout,
        sink_in,
        step_in,
        real_in,
        freq_in,
        in_re_in,
        in_im_in,
        out_re_in,
        out_im_in,
        skip_in,
        shift_in,
        out,
        sink,
        log_step,
        decay_real,
        decay_freq,
        in_re,
        in_im,
        out_re,
        out_im,
        skip_t,
        shift,
        h_ref,
        win,
        wkvq,
        wgate,
        who,
        wso,
        drive,
        cmat,
        skip_ref,
        bias,
        tri,
        grow,
        shrink,
        decay,
        pair_tile,
        u_ref,
        us_ref,
        es_ref,
        x_ref,
        s_ref,
        tot_re,
        tot_im,
        ent_re,
        ent_im,
        q_ref,
        kv_ref,
        hg_ref,
        sg_ref,
        hm_ref,
        sm_ref,
        acc_ref,
        psend,
        precv,
        s_buf,
        l_buf,
        zs_buf,
        zl_buf,
        pre,
        load_sem,
        h_sem,
        halo_sem,
        out_send,
        out_recv,
        s_send,
        s_recv,
        l_send,
        l_recv,
        zs_send,
        zs_recv,
        zl_send,
        zl_recv,
        ready_near,
        ready_far,
        ready_z,
    ) = refs
    sp, tp = lax.axis_index("sp"), lax.axis_index("tp")
    z, m = sp // plane, sp % plane
    other = 1 - tp

    apart = [k % nx + k // nx - (m % nx + m // nx) for k in range(plane)]
    behind = [
        jnp.logical_or(apart[k] > 0, jnp.logical_and(apart[k] == 0, k > m)) for k in range(plane)
    ]
    ahead = [
        jnp.logical_or(apart[k] < 0, jnp.logical_and(apart[k] == 0, k < m)) for k in range(plane)
    ]

    def count(conditions):
        return sum(condition.astype(jnp.int32) for condition in conditions)

    barrier = pltpu.get_barrier_semaphore()

    def signal(semaphore, device):
        pl.semaphore_signal(semaphore, inc=1, device_id=device, device_id_type=MESH)

    def when(condition, act, *args):
        pl.when(condition)(functools.partial(act, *args))

    crosses = jnp.logical_and(m == plane - 1, z < nz - 1)
    crossed = jnp.logical_and(m == 0, z > 0)
    signal(barrier, (sp, other))
    for k in range(plane):
        when(behind[k], signal, barrier, (z * plane + k, tp))
    for r in range(1, nz):
        when(z + r < nz, signal, barrier, (sp + r * plane, tp))
    when(crossed, signal, barrier, (sp - 1, tp))
    loads = []

    def load(src, dst):
        copy = pltpu.make_async_copy(src, dst, load_sem.at[len(loads)])
        copy.start()
        loads.append(copy)
        return copy

    def remote(src, dst, send, recv, device):
        return pltpu.make_async_remote_copy(
            src_ref=src,
            dst_ref=dst,
            send_sem=send,
            recv_sem=recv,
            device_id=device,
            device_id_type=MESH,
        )

    mine = pl.ds(pl.multiple_of(tp * HALF, HALF), HALF)
    theirs = pl.ds(pl.multiple_of(other * HALF, HALF), HALF)
    l_h = load(hidden, h_ref.at[:, mine])
    small = [
        load(src, dst)
        for src, dst in (
            (step_in, log_step),
            (real_in, decay_real),
            (freq_in, decay_freq),
            (shift_in, shift),
            (in_re_in, in_re),
            (in_im_in, in_im),
            (out_re_in, out_re),
            (out_im_in, out_im),
            (skip_in, skip_t),
            (sink_in, sink),
        )
    ]
    l_in = load(w_sin, win)

    row = lax.broadcasted_iota(jnp.int32, (TOK, TOK), 0)
    col = lax.broadcasted_iota(jnp.int32, (TOK, TOK), 1)
    tri[0:TOK, :] = ((row // SEG == col // SEG) & (col <= row)).astype(F32).astype(BF16)
    srow = lax.broadcasted_iota(jnp.int32, (CHUNKS, TOK), 0)
    scol = lax.broadcasted_iota(jnp.int32, (CHUNKS, TOK), 1)
    tri[TOK:, :] = (scol // SEG == srow).astype(F32).astype(BF16)
    drive[...] = jnp.zeros_like(drive)
    cmat[...] = jnp.zeros_like(cmat)
    qi = lax.rem(row, WINDOW)
    inside = (col > qi) & (col <= qi + WINDOW)
    bias[0] = jnp.where(inside & ((col >= WINDOW) | (sp > 0)), 0.0, -1e30)
    bias[1] = jnp.where(inside, 0.0, -1e30)

    pl.semaphore_wait(barrier, 1 + count(ahead) + z + count([crosses]))
    l_h.wait()
    send_h = remote(h_ref.at[:, mine], h_ref.at[:, mine], h_sem.at[0], h_sem.at[1], (sp, other))
    send_h.start()
    for k in range(plane):
        far = apart[k] <= -FAR
        when(far, signal, ready_far, (z * plane + k, tp))
        close = jnp.logical_and(ahead[k], jnp.logical_not(far))
        when(close, signal, ready_near, (z * plane + k, tp))
    for r in range(1, nz):
        when(z >= r, signal, ready_z, (sp - r * plane, tp))
    l_k = load(w_key, wkvq.at[:, 0:256])
    l_v = load(w_value, wkvq.at[:, 256:512])
    l_q = load(w_query, wkvq.at[:, 512:1024])

    for copy in small:
        copy.wait()
    low = lax.broadcasted_iota(jnp.int32, (PAIRS, 128), 1) < 64

    def paired(value):
        pair_tile[...] = jnp.concatenate([value, value], axis=1)
        even = pair_tile[pl.ds(0, PAIRS, stride=2), :]
        odd = pair_tile[pl.ds(1, PAIRS, stride=2), :]
        return jnp.where(low, even, odd)

    pair_row = lax.broadcasted_iota(jnp.int32, (PAIRS, 128), 0)
    step = jnp.zeros((PAIRS, 128), F32)
    for i in range(PAIRS):
        step = jnp.where(
            pair_row == i, jnp.where(low, log_step[2 * i], log_step[2 * i + 1]), step
        )
    step = jnp.exp(step)
    real, freq = paired(decay_real[...]), paired(decay_freq[...])
    magnitude, inverse = jnp.exp(real * step), jnp.exp(-(real * step))
    cosine, sine = jnp.cos(freq * step), jnp.sin(freq * step)
    base = (magnitude * cosine, magnitude * sine)
    base_inv = (inverse * cosine, -(inverse * sine))
    denominator = real * real + freq * freq
    less = base[0] - 1.0
    zoh = (
        (less * real + base[1] * freq) / denominator,
        (base[1] * real - less * freq) / denominator,
    )

    for i in range(PAIRS):
        factor = (zoh[0][i : i + 1, :], zoh[1][i : i + 1, :])
        first = (i % 4) * 32
        value = cmul(factor, tuple(jnp.concatenate([t[2 * i], t[2 * i + 1]], axis=1) for t in (in_re, in_im)))
        for part in (0, 1):
            cols = slice(i * 256 + part * 128, i * 256 + part * 128 + 128)
            drive[first : first + 16, cols] = jnp.where(low, value[part], 0.0).astype(BF16)
            drive[first + 16 : first + 32, cols] = jnp.where(low, 0.0, value[part]).astype(BF16)

    power = lax.broadcasted_iota(jnp.int32, (8, 128), 0) + 1
    ones, zeros = jnp.ones((8, 128), F32), jnp.zeros((8, 128), F32)

    def power_table(table, root):
        for i in range(PAIRS):
            b = tuple(jnp.broadcast_to(part[i : i + 1, :], (8, 128)) for part in root)
            value = (ones, zeros)
            for bit in range(4):
                has = (power >> bit) & 1 == 1
                value = cmul(value, (jnp.where(has, b[0], ones), jnp.where(has, b[1], zeros)))
                if bit < 3:
                    b = cmul(b, b)
            cols = slice(i * 128, i * 128 + 128)
            upper = cmul(value, b)
            for k in (0, 1):
                table[k, 0:8, cols] = value[k]
                table[k, 8:16, cols] = upper[k]
    power_table(shrink, base_inv)
    a_seg = csquares(base, log2(SEG))
    a_dev = csquares(a_seg, log2(CHUNKS))
    a_plane = csquares(a_dev, log2(plane))

    def shift_sums(mask):
        rest = jnp.broadcast_to(shift[...][:, None, :], (2 * PAIRS, 16, TOK)).reshape(512, TOK)
        sums = None
        for _ in range(3):
            part = rest.astype(BF16)
            term = dot_nt(mask, part)
            sums = term if sums is None else sums + term
            rest = rest - part.astype(F32)
        return sums

    es_ref[...] = shift_sums(tri[0:TOK, :])
    lane = lax.broadcasted_iota(jnp.int32, (PAIRS, 128), 1)
    total_shift = jnp.zeros((PAIRS, 128), F32)
    for c in range(CHUNKS):
        if c % 8 == 0:
            pair_tile[...] = shift[:, c * SEG : c * SEG + 128]
            even = pair_tile[pl.ds(0, PAIRS, stride=2), :]
            odd = pair_tile[pl.ds(1, PAIRS, stride=2), :]
        inside = lane // SEG == c % 8
        s = jnp.where(
            low,
            jnp.sum(jnp.where(inside, even, 0.0), axis=1, keepdims=True),
            jnp.sum(jnp.where(inside, odd, 0.0), axis=1, keepdims=True),
        )
        total_shift = total_shift + s
        decay[c] = jnp.exp(s)
    s_buf[m] = jnp.sum(
        jnp.where(lane % 64 == pair_row, total_shift, 0.0), axis=0, keepdims=True
    )

    l_in.wait()
    u_ref[...] = dot(h_ref[:, mine], win[mine, :])
    send_h.wait_recv()
    l_hg = load(w_hgate, wgate.at[:, 0:512])
    l_sg = load(w_sgate, wgate.at[:, 512:1024])
    l_ho = load(w_hout, who)
    l_so = load(w_sout, wso)
    u = (u_ref[...] + dot(h_ref[:, theirs], win[theirs, :])).astype(BF16).astype(F32)
    u_ref[...] = u
    us_ref[...] = (u * jnp.exp(-es_ref[...])).astype(BF16)

    def plane_copy(buf, send, recv, k):
        return remote(buf.at[m], buf.at[m], send.at[k], recv.at[m], (z * plane + k, tp))

    def plane_wait(buf, send, recv, k):
        remote(buf.at[k], buf.at[k], send.at[k], recv.at[k], (z * plane + k, tp)).wait_recv()

    for i in range(PAIRS):
        cols, narrow = slice(i * 256, i * 256 + 256), slice(i * 128, i * 128 + 128)
        j = i // 4
        push = dot(us_ref[:, j * 128 : j * 128 + 128], drive[:, cols])
        push = (push[:, :128].reshape(CHUNKS, SEG, 128), push[:, 128:].reshape(CHUNKS, SEG, 128))
        back = (shrink[0, :, narrow][None], shrink[1, :, narrow][None])
        w = cmul(push, back)
        w = jnp.concatenate([part.reshape(TOK, 128).astype(BF16) for part in w], axis=1)
        summed = dot(tri[...], w)
        x_ref[:, cols] = summed[:TOK]
        tot_re[i * 16 : i * 16 + 16, :] = summed[TOK:, :128]
        tot_im[i * 16 : i * 16 + 16, :] = summed[TOK:, 128:]

    flat_zero = jnp.zeros((PAIRS, 128), F32)
    flat_one = jnp.ones((PAIRS, 128), F32)

    def chunk_scan(state, keep):
        for c in range(CHUNKS):
            at = pl.ds(c, PAIRS, stride=CHUNKS)
            if keep:
                ent_re[at, :] = state[0]
                ent_im[at, :] = state[1]
            e = decay[c]
            state = cmul(
                (state[0] + tot_re[at, :], state[1] + tot_im[at, :]), (a_seg[0] * e, a_seg[1] * e)
            )
        return state

    state = chunk_scan((flat_zero, flat_zero), False)
    l_buf[m, 0] = state[0].astype(BF16)
    l_buf[m, 1] = state[1].astype(BF16)
    def send_to(k, condition):
        when(condition, plane_copy(l_buf, l_send, l_recv, k).start)
        when(condition, plane_copy(s_buf, s_send, s_recv, k).start)

    near = [jnp.logical_and(behind[k], apart[k] < FAR) for k in range(plane)]
    far = [apart[k] >= FAR for k in range(plane)]
    for k in range(plane):
        send_to(k, ahead[k])
    row_end = m % nx == nx - 1
    late = max(nz // 2 - 1, 1)
    late_cross = jnp.logical_and(m == plane - 1, z < late)
    late_halo = jnp.logical_and(m == 0, jnp.logical_and(z > 0, z <= late))
    l_k.wait()
    l_v.wait()
    halo = remote(
        kv_ref.at[TOK : TOK + WINDOW, :],
        kv_ref.at[0:WINDOW, :],
        halo_sem.at[0],
        halo_sem.at[1],
        (lax.rem(sp + 1, nz * plane), tp),
    )

    @pl.when(row_end)
    def _():
        kv_ref[TOK:, :] = dot(h_ref[WINDOW:, :], wkvq[:, 0:512]).astype(BF16)
    when(count(near) > 0, pl.semaphore_wait, ready_near, jnp.maximum(count(near), 1))
    for k in range(plane):
        send_to(k, near[k])
    early = jnp.logical_and(row_end, jnp.logical_or(m < plane - 1, z >= late))
    pl.when(jnp.logical_and(early, sp < nz * plane - 1))(halo.start)

    power_table(grow, base)
    for i in range(PAIRS):
        first = (i % 8) * 32
        value = [jnp.concatenate([t[2 * i], t[2 * i + 1]], axis=1) for t in (out_re, out_im)]
        value[1] = -value[1]
        for part in (0, 1):
            cols = slice(i * 256 + part * 128, i * 256 + part * 128 + 128)
            cmat[first : first + 16, cols] = jnp.where(low, value[part], 0.0).astype(BF16)
            cmat[first + 16 : first + 32, cols] = jnp.where(low, 0.0, value[part]).astype(BF16)
    channel = lax.broadcasted_iota(jnp.int32, (2 * PAIRS, 512), 1)
    group = lax.broadcasted_iota(jnp.int32, (2 * PAIRS, 512), 0)
    spread = (channel // 16 == group).astype(F32).astype(BF16)
    rest = skip_t[...]
    spread_skip = jnp.zeros((16, 512), F32)
    for _ in range(3):
        part = rest.astype(BF16)
        spread_skip = spread_skip + dot(part, spread)
        rest = rest - part.astype(F32)
    skip_ref[...] = jnp.sum(
        jnp.where((channel % 16 == group)[:16], spread_skip, 0.0), axis=0, keepdims=True
    )

    l_q.wait()
    rows = dot(h_ref[...], wkvq[...]).astype(BF16)
    kv_ref[WINDOW:TOK, :] = rows[0:WINDOW, 0:512]
    q_ref[...] = rows[:, 512:1024].astype(F32) * 0.125

    @pl.when(jnp.logical_not(row_end))
    def _():
        kv_ref[TOK:, :] = rows[WINDOW:, 0:512]

    pl.when(jnp.logical_not(row_end))(halo.start)
    when(count(far) > 0, pl.semaphore_wait, ready_far, jnp.maximum(count(far), 1))
    for k in range(plane):
        send_to(k, far[k])

    l_hg.wait()
    l_sg.wait()
    gates = jax.nn.sigmoid(dot(h_ref[...], wgate[...]).astype(BF16).astype(F32))
    hg_ref[...] = gates[:, 0:512]
    sg_ref[...] = gates[:, 512:1024]

    pl.when(late_cross)(halo.start)

    left = lax.broadcasted_iota(jnp.int32, (WINDOW, 128), 1) < 64

    def attend(n):
        rows = slice(n * WINDOW, (n + 1) * WINDOW)
        keys = slice(n * WINDOW, (n + 2) * WINDOW)
        for h in range(KV_HEADS):
            q = q_ref[rows, h * 128 : h * 128 + 128]
            turned = pltpu.roll(q, 64, 1)
            in_half = left if h % 2 == 0 else jnp.logical_not(left)
            first, second = (q, turned) if h % 2 == 0 else (turned, q)
            stacked = jnp.concatenate(
                [jnp.where(in_half, part, 0.0).astype(BF16) for part in (first, second)], axis=0
            )
            tile = slice((h // 2) * 128, (h // 2) * 128 + 128)
            scores = dot_nt(stacked, kv_ref[keys, tile]) + bias[n]
            first_row = lax.broadcasted_iota(jnp.int32, (2 * WINDOW, 1), 0) < WINDOW
            sink_col = jnp.where(first_row, sink[2 * h], sink[2 * h + 1])
            peak = jnp.maximum(jnp.max(scores, axis=1, keepdims=True), sink_col)
            e = jnp.exp(scores - peak)
            total = jnp.sum(e, axis=1, keepdims=True) + jnp.exp(sink_col - peak)
            vtile = slice(256 + (h // 2) * 128, 256 + (h // 2) * 128 + 128)
            mixed = dot(e.astype(BF16), kv_ref[keys, vtile]) / total
            a, b = mixed[:WINDOW], mixed[WINDOW:]
            if h % 2 == 0:
                joined = jnp.where(left, a, pltpu.roll(b, 64, 1))
            else:
                joined = jnp.where(left, pltpu.roll(a, 64, 1), b)
            gate = hg_ref[rows, h * 128 : h * 128 + 128]
            hm_ref[rows, h * 128 : h * 128 + 128] = (gate * joined).astype(BF16)
    attend(1)

    for k in range(plane):
        when(m != k, plane_wait, s_buf, s_send, s_recv, k)
        when(m != k, plane_wait, l_buf, l_send, l_recv, k)
    state, through = (flat_zero, flat_zero), (flat_one, flat_zero)
    before, before_through = state, through
    plane_shift = jnp.zeros((1, 128), F32)

    def spread_row(sums):
        own = jnp.where(lane % 64 == pair_row, sums, 0.0)
        return jnp.where(
            low,
            jnp.sum(jnp.where(low, own, 0.0), axis=1, keepdims=True),
            jnp.sum(jnp.where(low, 0.0, own), axis=1, keepdims=True),
        )

    for k in range(plane):
        here = m == k
        before = tuple(jnp.where(here, new, old) for new, old in zip(state, before))
        before_through = tuple(
            jnp.where(here, new, old) for new, old in zip(through, before_through)
        )
        e = jnp.exp(spread_row(s_buf[k]))
        factor = (a_dev[0] * e, a_dev[1] * e)
        through = cmul(factor, through)
        state = cmul(factor, state)
        state = (state[0] + l_buf[k, 0].astype(F32), state[1] + l_buf[k, 1].astype(F32))
        plane_shift = plane_shift + s_buf[k]
    zs_buf[z] = plane_shift
    zl_buf[z, 0] = state[0].astype(BF16)
    zl_buf[z, 1] = state[1].astype(BF16)
    when(z < nz - 1, pl.semaphore_wait, ready_z, nz - 1 - z)

    def z_copy(buf, send, recv, k):
        return remote(buf.at[z], buf.at[z], send.at[k], recv.at[z], (k * plane + m, tp))

    def z_wait(buf, send, recv, k):
        remote(buf.at[k], buf.at[k], send.at[k], recv.at[k], (k * plane + m, tp)).wait_recv()

    for k in range(nz - 1, 0, -1):
        when(z < k, z_copy(zl_buf, zl_send, zl_recv, k).start)
        when(z < k, z_copy(zs_buf, zs_send, zs_recv, k).start)

    l_ho.wait()

    def finish_heads():
        @pl.when(sp == 0)
        def _():
            kv_ref[0:WINDOW, :] = jnp.zeros((WINDOW, 512), BF16)

        pl.when(sp > 0)(halo.wait_recv)
        attend(0)
        acc_ref[...] = dot(hm_ref[...], who[...])

    pl.when(jnp.logical_not(late_halo))(finish_heads)

    pre[...] = jnp.zeros_like(pre)
    for k in range(nz - 1):

        @pl.when(k < z)
        def _(k=k):
            z_wait(zs_buf, zs_send, zs_recv, k)
            z_wait(zl_buf, zl_send, zl_recv, k)
            e = jnp.exp(spread_row(zs_buf[k]))
            new = cmul((a_plane[0] * e, a_plane[1] * e), (pre[0], pre[1]))
            pre[0] = new[0] + zl_buf[k, 0].astype(F32)
            pre[1] = new[1] + zl_buf[k, 1].astype(F32)

    carry = cmul(before_through, (pre[0], pre[1]))
    carry = (before[0] + carry[0], before[1] + carry[1])
    chunk_scan(carry, True)
    for half in (0, 1):
        for k in range(8):
            i = 8 * half + k
            narrow = slice(i * 128, i * 128 + 128)
            growth = (grow[0, :, narrow], grow[1, :, narrow])
            for c in range(CHUNKS):
                rows = slice(c * SEG, c * SEG + SEG)
                entry = i * CHUNKS + c
                re, im = slice(i * 256, i * 256 + 128), slice(i * 256 + 128, i * 256 + 256)
                state = (
                    x_ref[rows, re] + ent_re[entry : entry + 1, :],
                    x_ref[rows, im] + ent_im[entry : entry + 1, :],
                )
                state = cmul(state, growth)
                s_ref[rows, re] = state[0].astype(BF16)
                s_ref[rows, im] = state[1].astype(BF16)
        cols = slice(half * 256, half * 256 + 256)
        wide = slice(half * 2048, half * 2048 + 2048)
        rec = dot_nt(s_ref[:, wide], cmat[:, wide])
        rec = rec * jnp.exp(es_ref[:, cols]) + skip_ref[:, cols] * u_ref[:, cols]
        sm_ref[:, cols] = (sg_ref[:, cols] * jax.nn.gelu(rec)).astype(BF16)

    pl.when(late_halo)(finish_heads)

    l_so.wait()
    outs = []
    width = HALF // N_OUT
    for k in range(N_OUT):
        cols = pl.ds(pl.multiple_of(other * HALF + k * width, width), width)
        psend[k] = (acc_ref[:, cols] + dot(sm_ref[...], wso[:, cols])).astype(BF16)
        copy = remote(psend.at[k], precv.at[k], out_send.at[k], out_recv.at[k], (sp, other))
        copy.start()
        outs.append(copy)
    acc_ref[:, mine] = acc_ref[:, mine] + dot(sm_ref[...], wso[:, mine])
    for k in range(N_OUT):
        cols = pl.ds(pl.multiple_of(tp * HALF + k * width, width), width)
        outs[k].wait_recv()
        out[:, k * width : k * width + width] = (acc_ref[:, cols] + precv[k].astype(F32)).astype(BF16)

    send_h.wait_send()
    pl.when(sp < nz * plane - 1)(halo.wait_send)
    for copy in outs:
        copy.wait_send()
    for k in range(plane):
        when(m != k, plane_copy(s_buf, s_send, s_recv, k).wait_send)
        when(m != k, plane_copy(l_buf, l_send, l_recv, k).wait_send)
    for k in range(1, nz):
        when(z < k, z_copy(zs_buf, zs_send, zs_recv, k).wait_send)
        when(z < k, z_copy(zl_buf, zl_send, zl_recv, k).wait_send)


def on_device(
    sizes,
    hidden,
    query_weight,
    key_weight,
    value_weight,
    head_gate_weight,
    state_in_weight,
    state_gate_weight,
    sink_logit,
    decay_real,
    decay_frequency,
    log_step,
    input_real,
    input_imaginary,
    output_real,
    output_imaginary,
    skip_weight,
    decay_shift,
    head_out_weight,
    state_out_weight,
):
    nz, ny, nx = sizes
    vmem = pl.BlockSpec(memory_space=pltpu.VMEM)
    hbm = pl.BlockSpec(memory_space=pl.ANY)
    plane = ny * nx
    scratch = [
        ((2 * PAIRS, 64), F32),
        ((2 * PAIRS, 64), F32),
        ((2 * PAIRS, 16, 64), F32),
        ((2 * PAIRS, 16, 64), F32),
        ((2 * PAIRS, 16, 64), F32),
        ((2 * PAIRS, 16, 64), F32),
        ((16, 2 * PAIRS), F32),
        ((2 * PAIRS, TOK), F32),
        ((TOK, D), BF16),
        ((D, 512), BF16),
        ((D, 1024), BF16),
        ((D, 1024), BF16),
        ((512, D), BF16),
        ((512, D), BF16),
        ((128, LANES), BF16),
        ((256, LANES), BF16),
        ((1, 512), F32),
        ((2, TOK, TOK), F32),
        ((TOK + CHUNKS, TOK), BF16),
        ((2, SEG, PAIRS * 128), F32),
        ((2, SEG, PAIRS * 128), F32),
        ((CHUNKS, PAIRS, 128), F32),
        ((2 * PAIRS, 128), F32),
        ((TOK, 512), F32),
        ((TOK, 512), BF16),
        ((TOK, 512), F32),
        ((TOK, LANES), F32),
        ((TOK, LANES), BF16),
        ((PAIRS * CHUNKS, 128), F32),
        ((PAIRS * CHUNKS, 128), F32),
        ((PAIRS * CHUNKS, 128), F32),
        ((PAIRS * CHUNKS, 128), F32),
        ((TOK, 512), F32),
        ((TOK + WINDOW, 512), BF16),
        ((TOK, 512), F32),
        ((TOK, 512), F32),
        ((TOK, 512), BF16),
        ((TOK, 512), BF16),
        ((TOK, D), F32),
        ((N_OUT, TOK, HALF // N_OUT), BF16),
        ((N_OUT, TOK, HALF // N_OUT), BF16),
        ((plane, 1, 128), F32),
        ((plane, 2, PAIRS, 128), BF16),
        ((nz, 1, 128), F32),
        ((nz, 2, PAIRS, 128), BF16),
        ((2, PAIRS, 128), F32),
    ]
    dma = pltpu.SemaphoreType.DMA
    regular = pltpu.SemaphoreType.REGULAR
    return pl.pallas_call(
        functools.partial(kernel, sizes),
        out_shape=jax.ShapeDtypeStruct((TOK, HALF), BF16),
        in_specs=[hbm] * 19,
        out_specs=vmem,
        scratch_shapes=[pltpu.SMEM((8,), F32), pltpu.SMEM((2 * PAIRS,), F32)]
        + [pltpu.VMEM(shape, dtype) for shape, dtype in scratch]
        + [dma((19,)), dma((2,)), dma((2,)), dma((N_OUT,)), dma((N_OUT,))]
        + [dma((plane,))] * 4
        + [dma((nz,))] * 4
        + [regular] * 3,
        compiler_params=pltpu.CompilerParams(
            collective_id=0, has_side_effects=True, vmem_limit_bytes=48 * 1024 * 1024
        ),
        name="layer",
    )(
        *(
            pltpu.with_memory_space_constraint(array, pltpu.HBM)
            for array in (
                hidden,
                query_weight,
                key_weight,
                value_weight,
                head_gate_weight,
                state_in_weight,
                state_gate_weight,
                head_out_weight,
                state_out_weight,
                sink_logit,
                log_step,
                decay_real,
                decay_frequency,
                input_real.transpose(0, 2, 1),
                input_imaginary.transpose(0, 2, 1),
                output_real,
                output_imaginary,
                skip_weight.T,
                decay_shift,
            )
        )
    )


def solution(mesh):
    sizes = SP_SIZES[mesh.shape["sp"]]
    in_specs = (
        P("sp", "tp"),
        P(None, "tp"),
        P(None, "tp"),
        P(None, "tp"),
        P(None, "tp"),
        P(None, "tp"),
        P(None, "tp"),
        P("tp"),
        P("tp", None),
        P("tp", None),
        P("tp"),
        P("tp", None, None),
        P("tp", None, None),
        P("tp", None, None),
        P("tp", None, None),
        P("tp", None),
        P("tp", "sp"),
        P("tp", None),
        P("tp", None),
    )
    return jax.shard_map(
        functools.partial(on_device, sizes),
        mesh=mesh,
        in_specs=in_specs,
        out_specs=P("sp", "tp"),
        check_vma=False,
    )
```

```python
import functools

import jax
import jax.numpy as jnp
from jax import lax
from jax.experimental import pallas as pl
from jax.experimental.pallas import tpu as pltpu
from jax.sharding import PartitionSpec as P

MESH = pl.DeviceIdType.MESH
F32 = jnp.float32
BF16 = jnp.bfloat16

TOK = 256
D = 2048
HALF = D // 2
WINDOW = 128
SEG = 16
CHUNKS = TOK // SEG
PAIRS = 16
LANES = PAIRS * 256
KV_HEADS = 4
SP_SIZES = {128: (8, 4, 4), 8: (2, 2, 2)}

FAR = 3
N_OUT = 2


def dot(a, b):
    return jnp.dot(a, b, preferred_element_type=F32)


def dot_nt(a, b):
    return lax.dot_general(a, b, (((1,), (1,)), ((), ())), preferred_element_type=F32)


def cmul(a, b):
    return (a[0] * b[0] - a[1] * b[1], a[0] * b[1] + a[1] * b[0])


def csquares(a, times):
    for _ in range(times):
        a = cmul(a, a)
    return a


def log2(n):
    return n.bit_length() - 1


def kernel(sizes, *refs):
    nz, ny, nx = sizes
    plane = ny * nx
    (
        hidden,
        w_query,
        w_key,
        w_value,
        w_hgate,
        w_sin,
        w_sgate,
        w_hout,
        w_sout,
        sink_in,
        step_in,
        real_in,
        freq_in,
        in_re_in,
        in_im_in,
        out_re_in,
        out_im_in,
        skip_in,
        shift_in,
        out,
        sink,
        log_step,
        decay_real,
        decay_freq,
        in_re,
        in_im,
        out_re,
        out_im,
        skip_t,
        shift,
        h_ref,
        win,
        wkvq,
        wgate,
        who,
        wso,
        drive,
        cmat,
        skip_ref,
        bias,
        tri,
        grow,
        shrink,
        decay,
        pair_tile,
        u_ref,
        us_ref,
        es_ref,
        x_ref,
        s_ref,
        tot_re,
        tot_im,
        ent_re,
        ent_im,
        q_ref,
        kv_ref,
        hg_ref,
        sg_ref,
        hm_ref,
        sm_ref,
        acc_ref,
        psend,
        precv,
        s_buf,
        l_buf,
        zs_buf,
        zl_buf,
        pre,
        load_sem,
        h_sem,
        halo_sem,
        out_send,
        out_recv,
        s_send,
        s_recv,
        l_send,
        l_recv,
        zs_send,
        zs_recv,
        zl_send,
        zl_recv,
        ready_near,
        ready_far,
        ready_z,
    ) = refs
    sp, tp = lax.axis_index("sp"), lax.axis_index("tp")
    z, m = sp // plane, sp % plane
    other = 1 - tp

    apart = [k % nx + k // nx - (m % nx + m // nx) for k in range(plane)]
    behind = [
        jnp.logical_or(apart[k] > 0, jnp.logical_and(apart[k] == 0, k > m)) for k in range(plane)
    ]
    ahead = [
        jnp.logical_or(apart[k] < 0, jnp.logical_and(apart[k] == 0, k < m)) for k in range(plane)
    ]

    def count(conditions):
        return sum(condition.astype(jnp.int32) for condition in conditions)

    barrier = pltpu.get_barrier_semaphore()

    def signal(semaphore, device):
        pl.semaphore_signal(semaphore, inc=1, device_id=device, device_id_type=MESH)

    def when(condition, act, *args):
        pl.when(condition)(functools.partial(act, *args))

    crosses = jnp.logical_and(m == plane - 1, z < nz - 1)
    crossed = jnp.logical_and(m == 0, z > 0)
    signal(barrier, (sp, other))
    for k in range(plane):
        when(behind[k], signal, barrier, (z * plane + k, tp))
    for r in range(1, nz):
        when(z + r < nz, signal, barrier, (sp + r * plane, tp))
    when(crossed, signal, barrier, (sp - 1, tp))
    loads = []

    def load(src, dst):
        copy = pltpu.make_async_copy(src, dst, load_sem.at[len(loads)])
        copy.start()
        loads.append(copy)
        return copy

    def remote(src, dst, send, recv, device):
        return pltpu.make_async_remote_copy(
            src_ref=src,
            dst_ref=dst,
            send_sem=send,
            recv_sem=recv,
            device_id=device,
            device_id_type=MESH,
        )

    mine = pl.ds(pl.multiple_of(tp * HALF, HALF), HALF)
    theirs = pl.ds(pl.multiple_of(other * HALF, HALF), HALF)
    l_h = load(hidden, h_ref.at[:, mine])
    small = [
        load(src, dst)
        for src, dst in (
            (step_in, log_step),
            (real_in, decay_real),
            (freq_in, decay_freq),
            (shift_in, shift),
            (in_re_in, in_re),
            (in_im_in, in_im),
            (out_re_in, out_re),
            (out_im_in, out_im),
            (skip_in, skip_t),
            (sink_in, sink),
        )
    ]
    l_in = load(w_sin, win)

    row = lax.broadcasted_iota(jnp.int32, (TOK, TOK), 0)
    col = lax.broadcasted_iota(jnp.int32, (TOK, TOK), 1)
    tri[0:TOK, :] = ((row // SEG == col // SEG) & (col <= row)).astype(F32).astype(BF16)
    srow = lax.broadcasted_iota(jnp.int32, (CHUNKS, TOK), 0)
    scol = lax.broadcasted_iota(jnp.int32, (CHUNKS, TOK), 1)
    tri[TOK:, :] = (scol // SEG == srow).astype(F32).astype(BF16)
    drive[...] = jnp.zeros_like(drive)
    cmat[...] = jnp.zeros_like(cmat)
    qi = lax.rem(row, WINDOW)
    inside = (col > qi) & (col <= qi + WINDOW)
    bias[0] = jnp.where(inside & ((col >= WINDOW) | (sp > 0)), 0.0, -1e30)
    bias[1] = jnp.where(inside, 0.0, -1e30)

    pl.semaphore_wait(barrier, 1 + count(ahead) + z + count([crosses]))
    l_h.wait()
    send_h = remote(h_ref.at[:, mine], h_ref.at[:, mine], h_sem.at[0], h_sem.at[1], (sp, other))
    send_h.start()
    for k in range(plane):
        far = apart[k] <= -FAR
        when(far, signal, ready_far, (z * plane + k, tp))
        close = jnp.logical_and(ahead[k], jnp.logical_not(far))
        when(close, signal, ready_near, (z * plane + k, tp))
    for r in range(1, nz):
        when(z >= r, signal, ready_z, (sp - r * plane, tp))
    l_k = load(w_key, wkvq.at[:, 0:256])
    l_v = load(w_value, wkvq.at[:, 256:512])
    l_q = load(w_query, wkvq.at[:, 512:1024])

    for copy in small:
        copy.wait()
    low = lax.broadcasted_iota(jnp.int32, (PAIRS, 128), 1) < 64

    def paired(value):
        pair_tile[...] = jnp.concatenate([value, value], axis=1)
        even = pair_tile[pl.ds(0, PAIRS, stride=2), :]
        odd = pair_tile[pl.ds(1, PAIRS, stride=2), :]
        return jnp.where(low, even, odd)

    pair_row = lax.broadcasted_iota(jnp.int32, (PAIRS, 128), 0)
    step = jnp.zeros((PAIRS, 128), F32)
    for i in range(PAIRS):
        step = jnp.where(
            pair_row == i, jnp.where(low, log_step[2 * i], log_step[2 * i + 1]), step
        )
    step = jnp.exp(step)
    real, freq = paired(decay_real[...]), paired(decay_freq[...])
    magnitude, inverse = jnp.exp(real * step), jnp.exp(-(real * step))
    cosine, sine = jnp.cos(freq * step), jnp.sin(freq * step)
    base = (magnitude * cosine, magnitude * sine)
    base_inv = (inverse * cosine, -(inverse * sine))
    denominator = real * real + freq * freq
    less = base[0] - 1.0
    zoh = (
        (less * real + base[1] * freq) / denominator,
        (base[1] * real - less * freq) / denominator,
    )

    for i in range(PAIRS):
        factor = (zoh[0][i : i + 1, :], zoh[1][i : i + 1, :])
        first = (i % 4) * 32
        value = cmul(factor, tuple(jnp.concatenate([t[2 * i], t[2 * i + 1]], axis=1) for t in (in_re, in_im)))
        for part in (0, 1):
            cols = slice(i * 256 + part * 128, i * 256 + part * 128 + 128)
            drive[first : first + 16, cols] = jnp.where(low, value[part], 0.0).astype(BF16)
            drive[first + 16 : first + 32, cols] = jnp.where(low, 0.0, value[part]).astype(BF16)

    power = lax.broadcasted_iota(jnp.int32, (8, 128), 0) + 1
    ones, zeros = jnp.ones((8, 128), F32), jnp.zeros((8, 128), F32)

    def power_table(table, root):
        for i in range(PAIRS):
            b = tuple(jnp.broadcast_to(part[i : i + 1, :], (8, 128)) for part in root)
            value = (ones, zeros)
            for bit in range(4):
                has = (power >> bit) & 1 == 1
                value = cmul(value, (jnp.where(has, b[0], ones), jnp.where(has, b[1], zeros)))
                if bit < 3:
                    b = cmul(b, b)
            cols = slice(i * 128, i * 128 + 128)
            upper = cmul(value, b)
            for k in (0, 1):
                table[k, 0:8, cols] = value[k]
                table[k, 8:16, cols] = upper[k]
    power_table(shrink, base_inv)
    a_seg = csquares(base, log2(SEG))
    a_dev = csquares(a_seg, log2(CHUNKS))
    a_plane = csquares(a_dev, log2(plane))

    def shift_sums(mask):
        rest = jnp.broadcast_to(shift[...][:, None, :], (2 * PAIRS, 16, TOK)).reshape(512, TOK)
        sums = None
        for _ in range(3):
            part = rest.astype(BF16)
            term = dot_nt(mask, part)
            sums = term if sums is None else sums + term
            rest = rest - part.astype(F32)
        return sums

    es_ref[...] = shift_sums(tri[0:TOK, :])
    lane = lax.broadcasted_iota(jnp.int32, (PAIRS, 128), 1)
    total_shift = jnp.zeros((PAIRS, 128), F32)
    for c in range(CHUNKS):
        if c % 8 == 0:
            pair_tile[...] = shift[:, c * SEG : c * SEG + 128]
            even = pair_tile[pl.ds(0, PAIRS, stride=2), :]
            odd = pair_tile[pl.ds(1, PAIRS, stride=2), :]
        inside = lane // SEG == c % 8
        s = jnp.where(
            low,
            jnp.sum(jnp.where(inside, even, 0.0), axis=1, keepdims=True),
            jnp.sum(jnp.where(inside, odd, 0.0), axis=1, keepdims=True),
        )
        total_shift = total_shift + s
        decay[c] = jnp.exp(s)
    s_buf[m] = jnp.sum(
        jnp.where(lane % 64 == pair_row, total_shift, 0.0), axis=0, keepdims=True
    )

    l_in.wait()
    u_ref[...] = dot(h_ref[:, mine], win[mine, :])
    send_h.wait_recv()
    l_hg = load(w_hgate, wgate.at[:, 0:512])
    l_sg = load(w_sgate, wgate.at[:, 512:1024])
    l_ho = load(w_hout, who)
    l_so = load(w_sout, wso)
    u = (u_ref[...] + dot(h_ref[:, theirs], win[theirs, :])).astype(BF16).astype(F32)
    u_ref[...] = u
    us_ref[...] = (u * jnp.exp(-es_ref[...])).astype(BF16)

    def plane_copy(buf, send, recv, k):
        return remote(buf.at[m], buf.at[m], send.at[k], recv.at[m], (z * plane + k, tp))

    def plane_wait(buf, send, recv, k):
        remote(buf.at[k], buf.at[k], send.at[k], recv.at[k], (z * plane + k, tp)).wait_recv()

    for i in range(PAIRS):
        cols, narrow = slice(i * 256, i * 256 + 256), slice(i * 128, i * 128 + 128)
        j = i // 4
        push = dot(us_ref[:, j * 128 : j * 128 + 128], drive[:, cols])
        push = (push[:, :128].reshape(CHUNKS, SEG, 128), push[:, 128:].reshape(CHUNKS, SEG, 128))
        back = (shrink[0, :, narrow][None], shrink[1, :, narrow][None])
        w = cmul(push, back)
        w = jnp.concatenate([part.reshape(TOK, 128).astype(BF16) for part in w], axis=1)
        summed = dot(tri[...], w)
        x_ref[:, cols] = summed[:TOK]
        tot_re[i * 16 : i * 16 + 16, :] = summed[TOK:, :128]
        tot_im[i * 16 : i * 16 + 16, :] = summed[TOK:, 128:]

    flat_zero = jnp.zeros((PAIRS, 128), F32)
    flat_one = jnp.ones((PAIRS, 128), F32)

    def chunk_scan(state, keep):
        for c in range(CHUNKS):
            at = pl.ds(c, PAIRS, stride=CHUNKS)
            if keep:
                ent_re[at, :] = state[0]
                ent_im[at, :] = state[1]
            e = decay[c]
            state = cmul(
                (state[0] + tot_re[at, :], state[1] + tot_im[at, :]), (a_seg[0] * e, a_seg[1] * e)
            )
        return state

    state = chunk_scan((flat_zero, flat_zero), False)
    l_buf[m, 0] = state[0].astype(BF16)
    l_buf[m, 1] = state[1].astype(BF16)
    def send_to(k, condition):
        when(condition, plane_copy(l_buf, l_send, l_recv, k).start)
        when(condition, plane_copy(s_buf, s_send, s_recv, k).start)

    near = [jnp.logical_and(behind[k], apart[k] < FAR) for k in range(plane)]
    far = [apart[k] >= FAR for k in range(plane)]
    for k in range(plane):
        send_to(k, ahead[k])
    row_end = m % nx == nx - 1
    late = nz - 1
    late_cross = jnp.logical_and(m == plane - 1, z < late)
    late_halo = jnp.logical_and(m == 0, jnp.logical_and(z > 0, z <= late))
    l_k.wait()
    l_v.wait()
    halo = remote(
        kv_ref.at[TOK : TOK + WINDOW, :],
        kv_ref.at[0:WINDOW, :],
        halo_sem.at[0],
        halo_sem.at[1],
        (lax.rem(sp + 1, nz * plane), tp),
    )

    @pl.when(row_end)
    def _():
        kv_ref[TOK:, :] = dot(h_ref[WINDOW:, :], wkvq[:, 0:512]).astype(BF16)
    when(count(near) > 0, pl.semaphore_wait, ready_near, jnp.maximum(count(near), 1))
    for k in range(plane):
        send_to(k, near[k])
    early = jnp.logical_and(row_end, jnp.logical_or(m < plane - 1, z >= late))
    pl.when(jnp.logical_and(early, sp < nz * plane - 1))(halo.start)

    power_table(grow, base)
    for i in range(PAIRS):
        first = (i % 8) * 32
        value = [jnp.concatenate([t[2 * i], t[2 * i + 1]], axis=1) for t in (out_re, out_im)]
        value[1] = -value[1]
        for part in (0, 1):
            cols = slice(i * 256 + part * 128, i * 256 + part * 128 + 128)
            cmat[first : first + 16, cols] = jnp.where(low, value[part], 0.0).astype(BF16)
            cmat[first + 16 : first + 32, cols] = jnp.where(low, 0.0, value[part]).astype(BF16)
    channel = lax.broadcasted_iota(jnp.int32, (2 * PAIRS, 512), 1)
    group = lax.broadcasted_iota(jnp.int32, (2 * PAIRS, 512), 0)
    spread = (channel // 16 == group).astype(F32).astype(BF16)
    rest = skip_t[...]
    spread_skip = jnp.zeros((16, 512), F32)
    for _ in range(3):
        part = rest.astype(BF16)
        spread_skip = spread_skip + dot(part, spread)
        rest = rest - part.astype(F32)
    skip_ref[...] = jnp.sum(
        jnp.where((channel % 16 == group)[:16], spread_skip, 0.0), axis=0, keepdims=True
    )

    l_q.wait()
    rows = dot(h_ref[...], wkvq[...]).astype(BF16)
    kv_ref[WINDOW:TOK, :] = rows[0:WINDOW, 0:512]
    q_ref[...] = rows[:, 512:1024].astype(F32) * 0.125

    @pl.when(jnp.logical_not(row_end))
    def _():
        kv_ref[TOK:, :] = rows[WINDOW:, 0:512]

    pl.when(jnp.logical_not(row_end))(halo.start)
    when(count(far) > 0, pl.semaphore_wait, ready_far, jnp.maximum(count(far), 1))
    for k in range(plane):
        send_to(k, far[k])

    l_hg.wait()
    l_sg.wait()
    gates = jax.nn.sigmoid(dot(h_ref[...], wgate[...]).astype(BF16).astype(F32))
    hg_ref[...] = gates[:, 0:512]
    sg_ref[...] = gates[:, 512:1024]

    pl.when(late_cross)(halo.start)

    left = lax.broadcasted_iota(jnp.int32, (WINDOW, 128), 1) < 64

    def attend(n):
        rows = slice(n * WINDOW, (n + 1) * WINDOW)
        keys = slice(n * WINDOW, (n + 2) * WINDOW)
        for h in range(KV_HEADS):
            q = q_ref[rows, h * 128 : h * 128 + 128]
            turned = pltpu.roll(q, 64, 1)
            in_half = left if h % 2 == 0 else jnp.logical_not(left)
            first, second = (q, turned) if h % 2 == 0 else (turned, q)
            stacked = jnp.concatenate(
                [jnp.where(in_half, part, 0.0).astype(BF16) for part in (first, second)], axis=0
            )
            tile = slice((h // 2) * 128, (h // 2) * 128 + 128)
            scores = dot_nt(stacked, kv_ref[keys, tile]) + bias[n]
            first_row = lax.broadcasted_iota(jnp.int32, (2 * WINDOW, 1), 0) < WINDOW
            sink_col = jnp.where(first_row, sink[2 * h], sink[2 * h + 1])
            peak = jnp.maximum(jnp.max(scores, axis=1, keepdims=True), sink_col)
            e = jnp.exp(scores - peak)
            total = jnp.sum(e, axis=1, keepdims=True) + jnp.exp(sink_col - peak)
            vtile = slice(256 + (h // 2) * 128, 256 + (h // 2) * 128 + 128)
            mixed = dot(e.astype(BF16), kv_ref[keys, vtile]) / total
            a, b = mixed[:WINDOW], mixed[WINDOW:]
            if h % 2 == 0:
                joined = jnp.where(left, a, pltpu.roll(b, 64, 1))
            else:
                joined = jnp.where(left, pltpu.roll(a, 64, 1), b)
            gate = hg_ref[rows, h * 128 : h * 128 + 128]
            hm_ref[rows, h * 128 : h * 128 + 128] = (gate * joined).astype(BF16)
    attend(1)

    for k in range(plane):
        when(m != k, plane_wait, s_buf, s_send, s_recv, k)
        when(m != k, plane_wait, l_buf, l_send, l_recv, k)
    state, through = (flat_zero, flat_zero), (flat_one, flat_zero)
    before, before_through = state, through
    plane_shift = jnp.zeros((1, 128), F32)

    def spread_row(sums):
        own = jnp.where(lane % 64 == pair_row, sums, 0.0)
        return jnp.where(
            low,
            jnp.sum(jnp.where(low, own, 0.0), axis=1, keepdims=True),
            jnp.sum(jnp.where(low, 0.0, own), axis=1, keepdims=True),
        )

    for k in range(plane):
        here = m == k
        before = tuple(jnp.where(here, new, old) for new, old in zip(state, before))
        before_through = tuple(
            jnp.where(here, new, old) for new, old in zip(through, before_through)
        )
        e = jnp.exp(spread_row(s_buf[k]))
        factor = (a_dev[0] * e, a_dev[1] * e)
        through = cmul(factor, through)
        state = cmul(factor, state)
        state = (state[0] + l_buf[k, 0].astype(F32), state[1] + l_buf[k, 1].astype(F32))
        plane_shift = plane_shift + s_buf[k]
    zs_buf[z] = plane_shift
    zl_buf[z, 0] = state[0].astype(BF16)
    zl_buf[z, 1] = state[1].astype(BF16)
    when(z < nz - 1, pl.semaphore_wait, ready_z, nz - 1 - z)

    def z_copy(buf, send, recv, k):
        return remote(buf.at[z], buf.at[z], send.at[k], recv.at[z], (k * plane + m, tp))

    def z_wait(buf, send, recv, k):
        remote(buf.at[k], buf.at[k], send.at[k], recv.at[k], (k * plane + m, tp)).wait_recv()

    for k in range(nz - 1, 0, -1):
        when(z < k, z_copy(zl_buf, zl_send, zl_recv, k).start)
        when(z < k, z_copy(zs_buf, zs_send, zs_recv, k).start)

    l_ho.wait()

    def finish_heads():
        @pl.when(sp == 0)
        def _():
            kv_ref[0:WINDOW, :] = jnp.zeros((WINDOW, 512), BF16)

        pl.when(sp > 0)(halo.wait_recv)
        attend(0)
        acc_ref[...] = dot(hm_ref[...], who[...])

    pl.when(jnp.logical_not(late_halo))(finish_heads)

    pre[...] = jnp.zeros_like(pre)
    for k in range(nz - 1):

        @pl.when(k < z)
        def _(k=k):
            z_wait(zs_buf, zs_send, zs_recv, k)
            z_wait(zl_buf, zl_send, zl_recv, k)
            e = jnp.exp(spread_row(zs_buf[k]))
            new = cmul((a_plane[0] * e, a_plane[1] * e), (pre[0], pre[1]))
            pre[0] = new[0] + zl_buf[k, 0].astype(F32)
            pre[1] = new[1] + zl_buf[k, 1].astype(F32)

    carry = cmul(before_through, (pre[0], pre[1]))
    carry = (before[0] + carry[0], before[1] + carry[1])
    chunk_scan(carry, True)
    for half in (0, 1):
        for k in range(8):
            i = 8 * half + k
            narrow = slice(i * 128, i * 128 + 128)
            growth = (grow[0, :, narrow], grow[1, :, narrow])
            for c in range(CHUNKS):
                rows = slice(c * SEG, c * SEG + SEG)
                entry = i * CHUNKS + c
                re, im = slice(i * 256, i * 256 + 128), slice(i * 256 + 128, i * 256 + 256)
                state = (
                    x_ref[rows, re] + ent_re[entry : entry + 1, :],
                    x_ref[rows, im] + ent_im[entry : entry + 1, :],
                )
                state = cmul(state, growth)
                s_ref[rows, re] = state[0].astype(BF16)
                s_ref[rows, im] = state[1].astype(BF16)
        cols = slice(half * 256, half * 256 + 256)
        wide = slice(half * 2048, half * 2048 + 2048)
        rec = dot_nt(s_ref[:, wide], cmat[:, wide])
        rec = rec * jnp.exp(es_ref[:, cols]) + skip_ref[:, cols] * u_ref[:, cols]
        sm_ref[:, cols] = (sg_ref[:, cols] * jax.nn.gelu(rec)).astype(BF16)

    pl.when(late_halo)(finish_heads)

    l_so.wait()
    outs = []
    width = HALF // N_OUT
    for k in range(N_OUT):
        cols = pl.ds(pl.multiple_of(other * HALF + k * width, width), width)
        psend[k] = (acc_ref[:, cols] + dot(sm_ref[...], wso[:, cols])).astype(BF16)
        copy = remote(psend.at[k], precv.at[k], out_send.at[k], out_recv.at[k], (sp, other))
        copy.start()
        outs.append(copy)
    acc_ref[:, mine] = acc_ref[:, mine] + dot(sm_ref[...], wso[:, mine])
    for k in range(N_OUT):
        cols = pl.ds(pl.multiple_of(tp * HALF + k * width, width), width)
        outs[k].wait_recv()
        out[:, k * width : k * width + width] = (acc_ref[:, cols] + precv[k].astype(F32)).astype(BF16)

    send_h.wait_send()
    pl.when(sp < nz * plane - 1)(halo.wait_send)
    for copy in outs:
        copy.wait_send()
    for k in range(plane):
        when(m != k, plane_copy(s_buf, s_send, s_recv, k).wait_send)
        when(m != k, plane_copy(l_buf, l_send, l_recv, k).wait_send)
    for k in range(1, nz):
        when(z < k, z_copy(zs_buf, zs_send, zs_recv, k).wait_send)
        when(z < k, z_copy(zl_buf, zl_send, zl_recv, k).wait_send)


def on_device(
    sizes,
    hidden,
    query_weight,
    key_weight,
    value_weight,
    head_gate_weight,
    state_in_weight,
    state_gate_weight,
    sink_logit,
    decay_real,
    decay_frequency,
    log_step,
    input_real,
    input_imaginary,
    output_real,
    output_imaginary,
    skip_weight,
    decay_shift,
    head_out_weight,
    state_out_weight,
):
    nz, ny, nx = sizes
    vmem = pl.BlockSpec(memory_space=pltpu.VMEM)
    hbm = pl.BlockSpec(memory_space=pl.ANY)
    plane = ny * nx
    scratch = [
        ((2 * PAIRS, 64), F32),
        ((2 * PAIRS, 64), F32),
        ((2 * PAIRS, 16, 64), F32),
        ((2 * PAIRS, 16, 64), F32),
        ((2 * PAIRS, 16, 64), F32),
        ((2 * PAIRS, 16, 64), F32),
        ((16, 2 * PAIRS), F32),
        ((2 * PAIRS, TOK), F32),
        ((TOK, D), BF16),
        ((D, 512), BF16),
        ((D, 1024), BF16),
        ((D, 1024), BF16),
        ((512, D), BF16),
        ((512, D), BF16),
        ((128, LANES), BF16),
        ((256, LANES), BF16),
        ((1, 512), F32),
        ((2, TOK, TOK), F32),
        ((TOK + CHUNKS, TOK), BF16),
        ((2, SEG, PAIRS * 128), F32),
        ((2, SEG, PAIRS * 128), F32),
        ((CHUNKS, PAIRS, 128), F32),
        ((2 * PAIRS, 128), F32),
        ((TOK, 512), F32),
        ((TOK, 512), BF16),
        ((TOK, 512), F32),
        ((TOK, LANES), F32),
        ((TOK, LANES), BF16),
        ((PAIRS * CHUNKS, 128), F32),
        ((PAIRS * CHUNKS, 128), F32),
        ((PAIRS * CHUNKS, 128), F32),
        ((PAIRS * CHUNKS, 128), F32),
        ((TOK, 512), F32),
        ((TOK + WINDOW, 512), BF16),
        ((TOK, 512), F32),
        ((TOK, 512), F32),
        ((TOK, 512), BF16),
        ((TOK, 512), BF16),
        ((TOK, D), F32),
        ((N_OUT, TOK, HALF // N_OUT), BF16),
        ((N_OUT, TOK, HALF // N_OUT), BF16),
        ((plane, 1, 128), F32),
        ((plane, 2, PAIRS, 128), BF16),
        ((nz, 1, 128), F32),
        ((nz, 2, PAIRS, 128), BF16),
        ((2, PAIRS, 128), F32),
    ]
    dma = pltpu.SemaphoreType.DMA
    regular = pltpu.SemaphoreType.REGULAR
    return pl.pallas_call(
        functools.partial(kernel, sizes),
        out_shape=jax.ShapeDtypeStruct((TOK, HALF), BF16),
        in_specs=[hbm] * 19,
        out_specs=vmem,
        scratch_shapes=[pltpu.SMEM((8,), F32), pltpu.SMEM((2 * PAIRS,), F32)]
        + [pltpu.VMEM(shape, dtype) for shape, dtype in scratch]
        + [dma((19,)), dma((2,)), dma((2,)), dma((N_OUT,)), dma((N_OUT,))]
        + [dma((plane,))] * 4
        + [dma((nz,))] * 4
        + [regular] * 3,
        compiler_params=pltpu.CompilerParams(
            collective_id=0, has_side_effects=True, vmem_limit_bytes=48 * 1024 * 1024
        ),
        name="layer",
    )(
        *(
            pltpu.with_memory_space_constraint(array, pltpu.HBM)
            for array in (
                hidden,
                query_weight,
                key_weight,
                value_weight,
                head_gate_weight,
                state_in_weight,
                state_gate_weight,
                head_out_weight,
                state_out_weight,
                sink_logit,
                log_step,
                decay_real,
                decay_frequency,
                input_real.transpose(0, 2, 1),
                input_imaginary.transpose(0, 2, 1),
                output_real,
                output_imaginary,
                skip_weight.T,
                decay_shift,
            )
        )
    )


def solution(mesh):
    sizes = SP_SIZES[mesh.shape["sp"]]
    in_specs = (
        P("sp", "tp"),
        P(None, "tp"),
        P(None, "tp"),
        P(None, "tp"),
        P(None, "tp"),
        P(None, "tp"),
        P(None, "tp"),
        P("tp"),
        P("tp", None),
        P("tp", None),
        P("tp"),
        P("tp", None, None),
        P("tp", None, None),
        P("tp", None, None),
        P("tp", None, None),
        P("tp", None),
        P("tp", "sp"),
        P("tp", None),
        P("tp", None),
    )
    return jax.shard_map(
        functools.partial(on_device, sizes),
        mesh=mesh,
        in_specs=in_specs,
        out_specs=P("sp", "tp"),
        check_vma=False,
    )
```

```python
import functools

import jax
import jax.numpy as jnp
from jax import lax
from jax.experimental import pallas as pl
from jax.experimental.pallas import tpu as pltpu
from jax.sharding import PartitionSpec as P

MESH = pl.DeviceIdType.MESH
F32 = jnp.float32
BF16 = jnp.bfloat16

TOK = 256
D = 2048
HALF = D // 2
WINDOW = 128
SEG = 16
CHUNKS = TOK // SEG
PAIRS = 16
LANES = PAIRS * 256
KV_HEADS = 4
SP_SIZES = {128: (8, 4, 4), 8: (2, 2, 2)}

FAR = 3
N_OUT = 2


def dot(a, b):
    return jnp.dot(a, b, preferred_element_type=F32)


def dot_nt(a, b):
    return lax.dot_general(a, b, (((1,), (1,)), ((), ())), preferred_element_type=F32)


def cmul(a, b):
    return (a[0] * b[0] - a[1] * b[1], a[0] * b[1] + a[1] * b[0])


def csquares(a, times):
    for _ in range(times):
        a = cmul(a, a)
    return a


def log2(n):
    return n.bit_length() - 1


def kernel(sizes, *refs):
    nz, ny, nx = sizes
    plane = ny * nx
    (
        hidden,
        w_query,
        w_key,
        w_value,
        w_hgate,
        w_sin,
        w_sgate,
        w_hout,
        w_sout,
        sink_in,
        step_in,
        real_in,
        freq_in,
        in_re_in,
        in_im_in,
        out_re_in,
        out_im_in,
        skip_in,
        shift_in,
        out,
        sink,
        log_step,
        decay_real,
        decay_freq,
        in_re,
        in_im,
        out_re,
        out_im,
        skip_t,
        shift,
        h_ref,
        win,
        wkvq,
        wgate,
        who,
        wso,
        drive,
        cmat,
        skip_ref,
        bias,
        tri,
        grow,
        shrink,
        decay,
        pair_tile,
        u_ref,
        us_ref,
        es_ref,
        x_ref,
        s_ref,
        tot_re,
        tot_im,
        ent_re,
        ent_im,
        q_ref,
        kv_ref,
        hg_ref,
        sg_ref,
        hm_ref,
        sm_ref,
        acc_ref,
        psend,
        precv,
        s_buf,
        l_buf,
        zs_buf,
        zl_buf,
        pre,
        load_sem,
        h_sem,
        halo_sem,
        out_send,
        out_recv,
        s_send,
        s_recv,
        l_send,
        l_recv,
        zs_send,
        zs_recv,
        zl_send,
        zl_recv,
        ready_near,
        ready_far,
        ready_z,
    ) = refs
    sp, tp = lax.axis_index("sp"), lax.axis_index("tp")
    z, m = sp // plane, sp % plane
    other = 1 - tp

    apart = [k % nx + k // nx - (m % nx + m // nx) for k in range(plane)]
    behind = [
        jnp.logical_or(apart[k] > 0, jnp.logical_and(apart[k] == 0, k > m)) for k in range(plane)
    ]
    ahead = [
        jnp.logical_or(apart[k] < 0, jnp.logical_and(apart[k] == 0, k < m)) for k in range(plane)
    ]

    def count(conditions):
        return sum(condition.astype(jnp.int32) for condition in conditions)

    barrier = pltpu.get_barrier_semaphore()

    def signal(semaphore, device):
        pl.semaphore_signal(semaphore, inc=1, device_id=device, device_id_type=MESH)

    def when(condition, act, *args):
        pl.when(condition)(functools.partial(act, *args))

    crosses = jnp.logical_and(m == plane - 1, z < nz - 1)
    crossed = jnp.logical_and(m == 0, z > 0)
    signal(barrier, (sp, other))
    for k in range(plane):
        when(behind[k], signal, barrier, (z * plane + k, tp))
    for r in range(1, nz):
        when(z + r < nz, signal, barrier, (sp + r * plane, tp))
    when(crossed, signal, barrier, (sp - 1, tp))
    loads = []

    def load(src, dst):
        copy = pltpu.make_async_copy(src, dst, load_sem.at[len(loads)])
        copy.start()
        loads.append(copy)
        return copy

    def remote(src, dst, send, recv, device):
        return pltpu.make_async_remote_copy(
            src_ref=src,
            dst_ref=dst,
            send_sem=send,
            recv_sem=recv,
            device_id=device,
            device_id_type=MESH,
        )

    mine = pl.ds(pl.multiple_of(tp * HALF, HALF), HALF)
    theirs = pl.ds(pl.multiple_of(other * HALF, HALF), HALF)
    l_h = load(hidden, h_ref.at[:, mine])
    small = [
        load(src, dst)
        for src, dst in (
            (step_in, log_step),
            (real_in, decay_real),
            (freq_in, decay_freq),
            (shift_in, shift),
            (in_re_in, in_re),
            (in_im_in, in_im),
            (out_re_in, out_re),
            (out_im_in, out_im),
            (skip_in, skip_t),
            (sink_in, sink),
        )
    ]
    l_in = load(w_sin, win)

    row = lax.broadcasted_iota(jnp.int32, (TOK, TOK), 0)
    col = lax.broadcasted_iota(jnp.int32, (TOK, TOK), 1)
    tri[0:TOK, :] = ((row // SEG == col // SEG) & (col <= row)).astype(F32).astype(BF16)
    srow = lax.broadcasted_iota(jnp.int32, (CHUNKS, TOK), 0)
    scol = lax.broadcasted_iota(jnp.int32, (CHUNKS, TOK), 1)
    tri[TOK:, :] = (scol // SEG == srow).astype(F32).astype(BF16)
    drive[...] = jnp.zeros_like(drive)
    cmat[...] = jnp.zeros_like(cmat)
    qi = lax.rem(row, WINDOW)
    inside = (col > qi) & (col <= qi + WINDOW)
    bias[0] = jnp.where(inside & ((col >= WINDOW) | (sp > 0)), 0.0, -1e30)
    bias[1] = jnp.where(inside, 0.0, -1e30)

    pl.semaphore_wait(barrier, 1 + count(ahead) + z + count([crosses]))
    l_h.wait()
    send_h = remote(h_ref.at[:, mine], h_ref.at[:, mine], h_sem.at[0], h_sem.at[1], (sp, other))
    send_h.start()
    for k in range(plane):
        far = apart[k] <= -FAR
        when(far, signal, ready_far, (z * plane + k, tp))
        close = jnp.logical_and(ahead[k], jnp.logical_not(far))
        when(close, signal, ready_near, (z * plane + k, tp))
    for r in range(1, nz):
        when(z >= r, signal, ready_z, (sp - r * plane, tp))
    l_k = load(w_key, wkvq.at[:, 0:256])
    l_v = load(w_value, wkvq.at[:, 256:512])
    l_q = load(w_query, wkvq.at[:, 512:1024])

    for copy in small:
        copy.wait()
    low = lax.broadcasted_iota(jnp.int32, (PAIRS, 128), 1) < 64

    def paired(value):
        pair_tile[...] = jnp.concatenate([value, value], axis=1)
        even = pair_tile[pl.ds(0, PAIRS, stride=2), :]
        odd = pair_tile[pl.ds(1, PAIRS, stride=2), :]
        return jnp.where(low, even, odd)

    pair_row = lax.broadcasted_iota(jnp.int32, (PAIRS, 128), 0)
    step = jnp.zeros((PAIRS, 128), F32)
    for i in range(PAIRS):
        step = jnp.where(
            pair_row == i, jnp.where(low, log_step[2 * i], log_step[2 * i + 1]), step
        )
    step = jnp.exp(step)
    real, freq = paired(decay_real[...]), paired(decay_freq[...])
    magnitude, inverse = jnp.exp(real * step), jnp.exp(-(real * step))
    cosine, sine = jnp.cos(freq * step), jnp.sin(freq * step)
    base = (magnitude * cosine, magnitude * sine)
    base_inv = (inverse * cosine, -(inverse * sine))
    denominator = real * real + freq * freq
    less = base[0] - 1.0
    zoh = (
        (less * real + base[1] * freq) / denominator,
        (base[1] * real - less * freq) / denominator,
    )

    for i in range(PAIRS):
        factor = (zoh[0][i : i + 1, :], zoh[1][i : i + 1, :])
        first = (i % 4) * 32
        value = cmul(factor, tuple(jnp.concatenate([t[2 * i], t[2 * i + 1]], axis=1) for t in (in_re, in_im)))
        for part in (0, 1):
            cols = slice(i * 256 + part * 128, i * 256 + part * 128 + 128)
            drive[first : first + 16, cols] = jnp.where(low, value[part], 0.0).astype(BF16)
            drive[first + 16 : first + 32, cols] = jnp.where(low, 0.0, value[part]).astype(BF16)

    power = lax.broadcasted_iota(jnp.int32, (8, 128), 0) + 1
    ones, zeros = jnp.ones((8, 128), F32), jnp.zeros((8, 128), F32)

    def power_table(table, root):
        for i in range(PAIRS):
            b = tuple(jnp.broadcast_to(part[i : i + 1, :], (8, 128)) for part in root)
            value = (ones, zeros)
            for bit in range(4):
                has = (power >> bit) & 1 == 1
                value = cmul(value, (jnp.where(has, b[0], ones), jnp.where(has, b[1], zeros)))
                if bit < 3:
                    b = cmul(b, b)
            cols = slice(i * 128, i * 128 + 128)
            upper = cmul(value, b)
            for k in (0, 1):
                table[k, 0:8, cols] = value[k]
                table[k, 8:16, cols] = upper[k]
    power_table(shrink, base_inv)
    a_seg = csquares(base, log2(SEG))
    a_dev = csquares(a_seg, log2(CHUNKS))
    a_plane = csquares(a_dev, log2(plane))

    def shift_sums(mask):
        rest = jnp.broadcast_to(shift[...][:, None, :], (2 * PAIRS, 16, TOK)).reshape(512, TOK)
        sums = None
        for _ in range(3):
            part = rest.astype(BF16)
            term = dot_nt(mask, part)
            sums = term if sums is None else sums + term
            rest = rest - part.astype(F32)
        return sums

    es_ref[...] = shift_sums(tri[0:TOK, :])
    lane = lax.broadcasted_iota(jnp.int32, (PAIRS, 128), 1)
    total_shift = jnp.zeros((PAIRS, 128), F32)
    for c in range(CHUNKS):
        if c % 8 == 0:
            pair_tile[...] = shift[:, c * SEG : c * SEG + 128]
            even = pair_tile[pl.ds(0, PAIRS, stride=2), :]
            odd = pair_tile[pl.ds(1, PAIRS, stride=2), :]
        inside = lane // SEG == c % 8
        s = jnp.where(
            low,
            jnp.sum(jnp.where(inside, even, 0.0), axis=1, keepdims=True),
            jnp.sum(jnp.where(inside, odd, 0.0), axis=1, keepdims=True),
        )
        total_shift = total_shift + s
        decay[c] = jnp.exp(s)
    s_buf[m] = jnp.sum(
        jnp.where(lane % 64 == pair_row, total_shift, 0.0), axis=0, keepdims=True
    )

    l_in.wait()
    u_ref[...] = dot(h_ref[:, mine], win[mine, :])
    send_h.wait_recv()
    l_hg = load(w_hgate, wgate.at[:, 0:512])
    l_sg = load(w_sgate, wgate.at[:, 512:1024])
    l_ho = load(w_hout, who)
    l_so = load(w_sout, wso)
    u = (u_ref[...] + dot(h_ref[:, theirs], win[theirs, :])).astype(BF16).astype(F32)
    u_ref[...] = u
    us_ref[...] = (u * jnp.exp(-es_ref[...])).astype(BF16)

    def plane_copy(buf, send, recv, k):
        return remote(buf.at[m], buf.at[m], send.at[k], recv.at[m], (z * plane + k, tp))

    def plane_wait(buf, send, recv, k):
        remote(buf.at[k], buf.at[k], send.at[k], recv.at[k], (z * plane + k, tp)).wait_recv()

    for i in range(PAIRS):
        cols, narrow = slice(i * 256, i * 256 + 256), slice(i * 128, i * 128 + 128)
        j = i // 4
        push = dot(us_ref[:, j * 128 : j * 128 + 128], drive[:, cols])
        push = (push[:, :128].reshape(CHUNKS, SEG, 128), push[:, 128:].reshape(CHUNKS, SEG, 128))
        back = (shrink[0, :, narrow][None], shrink[1, :, narrow][None])
        w = cmul(push, back)
        w = jnp.concatenate([part.reshape(TOK, 128).astype(BF16) for part in w], axis=1)
        summed = dot(tri[...], w)
        x_ref[:, cols] = summed[:TOK]
        tot_re[i * 16 : i * 16 + 16, :] = summed[TOK:, :128]
        tot_im[i * 16 : i * 16 + 16, :] = summed[TOK:, 128:]

    flat_zero = jnp.zeros((PAIRS, 128), F32)
    flat_one = jnp.ones((PAIRS, 128), F32)

    def chunk_scan(state, keep):
        for c in range(CHUNKS):
            at = pl.ds(c, PAIRS, stride=CHUNKS)
            if keep:
                ent_re[at, :] = state[0]
                ent_im[at, :] = state[1]
            e = decay[c]
            state = cmul(
                (state[0] + tot_re[at, :], state[1] + tot_im[at, :]), (a_seg[0] * e, a_seg[1] * e)
            )
        return state

    state = chunk_scan((flat_zero, flat_zero), False)
    l_buf[m, 0] = state[0].astype(BF16)
    l_buf[m, 1] = state[1].astype(BF16)
    def send_to(k, condition):
        when(condition, plane_copy(l_buf, l_send, l_recv, k).start)
        when(condition, plane_copy(s_buf, s_send, s_recv, k).start)

    near = [jnp.logical_and(behind[k], apart[k] < FAR) for k in range(plane)]
    far = [apart[k] >= FAR for k in range(plane)]
    for k in range(plane):
        send_to(k, ahead[k])
    row_end = m % nx == nx - 1
    late = max(nz // 2 - 1, 1)
    late_cross = jnp.logical_and(m == plane - 1, z < late)
    late_halo = jnp.logical_and(m == 0, jnp.logical_and(z > 0, z <= late))
    l_k.wait()
    l_v.wait()
    halo = remote(
        kv_ref.at[TOK : TOK + WINDOW, :],
        kv_ref.at[0:WINDOW, :],
        halo_sem.at[0],
        halo_sem.at[1],
        (lax.rem(sp + 1, nz * plane), tp),
    )

    @pl.when(row_end)
    def _():
        kv_ref[TOK:, :] = dot(h_ref[WINDOW:, :], wkvq[:, 0:512]).astype(BF16)
    when(count(near) > 0, pl.semaphore_wait, ready_near, jnp.maximum(count(near), 1))
    for k in range(plane):
        send_to(k, near[k])
    pl.when(jnp.logical_and(row_end, m < plane - 1))(halo.start)

    power_table(grow, base)
    for i in range(PAIRS):
        first = (i % 8) * 32
        value = [jnp.concatenate([t[2 * i], t[2 * i + 1]], axis=1) for t in (out_re, out_im)]
        value[1] = -value[1]
        for part in (0, 1):
            cols = slice(i * 256 + part * 128, i * 256 + part * 128 + 128)
            cmat[first : first + 16, cols] = jnp.where(low, value[part], 0.0).astype(BF16)
            cmat[first + 16 : first + 32, cols] = jnp.where(low, 0.0, value[part]).astype(BF16)
    channel = lax.broadcasted_iota(jnp.int32, (2 * PAIRS, 512), 1)
    group = lax.broadcasted_iota(jnp.int32, (2 * PAIRS, 512), 0)
    spread = (channel // 16 == group).astype(F32).astype(BF16)
    rest = skip_t[...]
    spread_skip = jnp.zeros((16, 512), F32)
    for _ in range(3):
        part = rest.astype(BF16)
        spread_skip = spread_skip + dot(part, spread)
        rest = rest - part.astype(F32)
    skip_ref[...] = jnp.sum(
        jnp.where((channel % 16 == group)[:16], spread_skip, 0.0), axis=0, keepdims=True
    )

    l_q.wait()
    rows = dot(h_ref[...], wkvq[...]).astype(BF16)
    kv_ref[WINDOW:TOK, :] = rows[0:WINDOW, 0:512]
    q_ref[...] = rows[:, 512:1024].astype(F32) * 0.125

    @pl.when(jnp.logical_not(row_end))
    def _():
        kv_ref[TOK:, :] = rows[WINDOW:, 0:512]

    soon = jnp.logical_and(crosses, z >= late)
    pl.when(jnp.logical_or(jnp.logical_not(row_end), soon))(halo.start)
    when(count(far) > 0, pl.semaphore_wait, ready_far, jnp.maximum(count(far), 1))
    for k in range(plane):
        send_to(k, far[k])

    l_hg.wait()
    l_sg.wait()
    gates = jax.nn.sigmoid(dot(h_ref[...], wgate[...]).astype(BF16).astype(F32))
    hg_ref[...] = gates[:, 0:512]
    sg_ref[...] = gates[:, 512:1024]

    pl.when(late_cross)(halo.start)

    left = lax.broadcasted_iota(jnp.int32, (WINDOW, 128), 1) < 64

    def attend(n):
        rows = slice(n * WINDOW, (n + 1) * WINDOW)
        keys = slice(n * WINDOW, (n + 2) * WINDOW)
        for h in range(KV_HEADS):
            q = q_ref[rows, h * 128 : h * 128 + 128]
            turned = pltpu.roll(q, 64, 1)
            in_half = left if h % 2 == 0 else jnp.logical_not(left)
            first, second = (q, turned) if h % 2 == 0 else (turned, q)
            stacked = jnp.concatenate(
                [jnp.where(in_half, part, 0.0).astype(BF16) for part in (first, second)], axis=0
            )
            tile = slice((h // 2) * 128, (h // 2) * 128 + 128)
            scores = dot_nt(stacked, kv_ref[keys, tile]) + bias[n]
            first_row = lax.broadcasted_iota(jnp.int32, (2 * WINDOW, 1), 0) < WINDOW
            sink_col = jnp.where(first_row, sink[2 * h], sink[2 * h + 1])
            peak = jnp.maximum(jnp.max(scores, axis=1, keepdims=True), sink_col)
            e = jnp.exp(scores - peak)
            total = jnp.sum(e, axis=1, keepdims=True) + jnp.exp(sink_col - peak)
            vtile = slice(256 + (h // 2) * 128, 256 + (h // 2) * 128 + 128)
            mixed = dot(e.astype(BF16), kv_ref[keys, vtile]) / total
            a, b = mixed[:WINDOW], mixed[WINDOW:]
            if h % 2 == 0:
                joined = jnp.where(left, a, pltpu.roll(b, 64, 1))
            else:
                joined = jnp.where(left, pltpu.roll(a, 64, 1), b)
            gate = hg_ref[rows, h * 128 : h * 128 + 128]
            hm_ref[rows, h * 128 : h * 128 + 128] = (gate * joined).astype(BF16)
    attend(1)

    for k in range(plane):
        when(m != k, plane_wait, s_buf, s_send, s_recv, k)
        when(m != k, plane_wait, l_buf, l_send, l_recv, k)
    state, through = (flat_zero, flat_zero), (flat_one, flat_zero)
    before, before_through = state, through
    plane_shift = jnp.zeros((1, 128), F32)

    def spread_row(sums):
        own = jnp.where(lane % 64 == pair_row, sums, 0.0)
        return jnp.where(
            low,
            jnp.sum(jnp.where(low, own, 0.0), axis=1, keepdims=True),
            jnp.sum(jnp.where(low, 0.0, own), axis=1, keepdims=True),
        )

    for k in range(plane):
        here = m == k
        before = tuple(jnp.where(here, new, old) for new, old in zip(state, before))
        before_through = tuple(
            jnp.where(here, new, old) for new, old in zip(through, before_through)
        )
        e = jnp.exp(spread_row(s_buf[k]))
        factor = (a_dev[0] * e, a_dev[1] * e)
        through = cmul(factor, through)
        state = cmul(factor, state)
        state = (state[0] + l_buf[k, 0].astype(F32), state[1] + l_buf[k, 1].astype(F32))
        plane_shift = plane_shift + s_buf[k]
    zs_buf[z] = plane_shift
    zl_buf[z, 0] = state[0].astype(BF16)
    zl_buf[z, 1] = state[1].astype(BF16)
    when(z < nz - 1, pl.semaphore_wait, ready_z, nz - 1 - z)

    def z_copy(buf, send, recv, k):
        return remote(buf.at[z], buf.at[z], send.at[k], recv.at[z], (k * plane + m, tp))

    def z_wait(buf, send, recv, k):
        remote(buf.at[k], buf.at[k], send.at[k], recv.at[k], (k * plane + m, tp)).wait_recv()

    for k in range(nz - 1, 0, -1):
        when(z < k, z_copy(zl_buf, zl_send, zl_recv, k).start)
        when(z < k, z_copy(zs_buf, zs_send, zs_recv, k).start)

    l_ho.wait()

    def finish_heads():
        @pl.when(sp == 0)
        def _():
            kv_ref[0:WINDOW, :] = jnp.zeros((WINDOW, 512), BF16)

        pl.when(sp > 0)(halo.wait_recv)
        attend(0)
        acc_ref[...] = dot(hm_ref[...], who[...])

    pl.when(jnp.logical_not(late_halo))(finish_heads)

    pre[...] = jnp.zeros_like(pre)
    for k in range(nz - 1):

        @pl.when(k < z)
        def _(k=k):
            z_wait(zs_buf, zs_send, zs_recv, k)
            z_wait(zl_buf, zl_send, zl_recv, k)
            e = jnp.exp(spread_row(zs_buf[k]))
            new = cmul((a_plane[0] * e, a_plane[1] * e), (pre[0], pre[1]))
            pre[0] = new[0] + zl_buf[k, 0].astype(F32)
            pre[1] = new[1] + zl_buf[k, 1].astype(F32)

    carry = cmul(before_through, (pre[0], pre[1]))
    carry = (before[0] + carry[0], before[1] + carry[1])
    chunk_scan(carry, True)
    for half in (0, 1):
        for k in range(8):
            i = 8 * half + k
            narrow = slice(i * 128, i * 128 + 128)
            growth = (grow[0, :, narrow], grow[1, :, narrow])
            for c in range(CHUNKS):
                rows = slice(c * SEG, c * SEG + SEG)
                entry = i * CHUNKS + c
                re, im = slice(i * 256, i * 256 + 128), slice(i * 256 + 128, i * 256 + 256)
                state = (
                    x_ref[rows, re] + ent_re[entry : entry + 1, :],
                    x_ref[rows, im] + ent_im[entry : entry + 1, :],
                )
                state = cmul(state, growth)
                s_ref[rows, re] = state[0].astype(BF16)
                s_ref[rows, im] = state[1].astype(BF16)
        cols = slice(half * 256, half * 256 + 256)
        wide = slice(half * 2048, half * 2048 + 2048)
        rec = dot_nt(s_ref[:, wide], cmat[:, wide])
        rec = rec * jnp.exp(es_ref[:, cols]) + skip_ref[:, cols] * u_ref[:, cols]
        sm_ref[:, cols] = (sg_ref[:, cols] * jax.nn.gelu(rec)).astype(BF16)

    pl.when(late_halo)(finish_heads)

    l_so.wait()
    outs = []
    width = HALF // N_OUT
    for k in range(N_OUT):
        cols = pl.ds(pl.multiple_of(other * HALF + k * width, width), width)
        psend[k] = (acc_ref[:, cols] + dot(sm_ref[...], wso[:, cols])).astype(BF16)
        copy = remote(psend.at[k], precv.at[k], out_send.at[k], out_recv.at[k], (sp, other))
        copy.start()
        outs.append(copy)
    acc_ref[:, mine] = acc_ref[:, mine] + dot(sm_ref[...], wso[:, mine])
    for k in range(N_OUT):
        cols = pl.ds(pl.multiple_of(tp * HALF + k * width, width), width)
        outs[k].wait_recv()
        out[:, k * width : k * width + width] = (acc_ref[:, cols] + precv[k].astype(F32)).astype(BF16)

    send_h.wait_send()
    pl.when(sp < nz * plane - 1)(halo.wait_send)
    for copy in outs:
        copy.wait_send()
    for k in range(plane):
        when(m != k, plane_copy(s_buf, s_send, s_recv, k).wait_send)
        when(m != k, plane_copy(l_buf, l_send, l_recv, k).wait_send)
    for k in range(1, nz):
        when(z < k, z_copy(zs_buf, zs_send, zs_recv, k).wait_send)
        when(z < k, z_copy(zl_buf, zl_send, zl_recv, k).wait_send)


def on_device(
    sizes,
    hidden,
    query_weight,
    key_weight,
    value_weight,
    head_gate_weight,
    state_in_weight,
    state_gate_weight,
    sink_logit,
    decay_real,
    decay_frequency,
    log_step,
    input_real,
    input_imaginary,
    output_real,
    output_imaginary,
    skip_weight,
    decay_shift,
    head_out_weight,
    state_out_weight,
):
    nz, ny, nx = sizes
    vmem = pl.BlockSpec(memory_space=pltpu.VMEM)
    hbm = pl.BlockSpec(memory_space=pl.ANY)
    plane = ny * nx
    scratch = [
        ((2 * PAIRS, 64), F32),
        ((2 * PAIRS, 64), F32),
        ((2 * PAIRS, 16, 64), F32),
        ((2 * PAIRS, 16, 64), F32),
        ((2 * PAIRS, 16, 64), F32),
        ((2 * PAIRS, 16, 64), F32),
        ((16, 2 * PAIRS), F32),
        ((2 * PAIRS, TOK), F32),
        ((TOK, D), BF16),
        ((D, 512), BF16),
        ((D, 1024), BF16),
        ((D, 1024), BF16),
        ((512, D), BF16),
        ((512, D), BF16),
        ((128, LANES), BF16),
        ((256, LANES), BF16),
        ((1, 512), F32),
        ((2, TOK, TOK), F32),
        ((TOK + CHUNKS, TOK), BF16),
        ((2, SEG, PAIRS * 128), F32),
        ((2, SEG, PAIRS * 128), F32),
        ((CHUNKS, PAIRS, 128), F32),
        ((2 * PAIRS, 128), F32),
        ((TOK, 512), F32),
        ((TOK, 512), BF16),
        ((TOK, 512), F32),
        ((TOK, LANES), F32),
        ((TOK, LANES), BF16),
        ((PAIRS * CHUNKS, 128), F32),
        ((PAIRS * CHUNKS, 128), F32),
        ((PAIRS * CHUNKS, 128), F32),
        ((PAIRS * CHUNKS, 128), F32),
        ((TOK, 512), F32),
        ((TOK + WINDOW, 512), BF16),
        ((TOK, 512), F32),
        ((TOK, 512), F32),
        ((TOK, 512), BF16),
        ((TOK, 512), BF16),
        ((TOK, D), F32),
        ((N_OUT, TOK, HALF // N_OUT), BF16),
        ((N_OUT, TOK, HALF // N_OUT), BF16),
        ((plane, 1, 128), F32),
        ((plane, 2, PAIRS, 128), BF16),
        ((nz, 1, 128), F32),
        ((nz, 2, PAIRS, 128), BF16),
        ((2, PAIRS, 128), F32),
    ]
    dma = pltpu.SemaphoreType.DMA
    regular = pltpu.SemaphoreType.REGULAR
    return pl.pallas_call(
        functools.partial(kernel, sizes),
        out_shape=jax.ShapeDtypeStruct((TOK, HALF), BF16),
        in_specs=[hbm] * 19,
        out_specs=vmem,
        scratch_shapes=[pltpu.SMEM((8,), F32), pltpu.SMEM((2 * PAIRS,), F32)]
        + [pltpu.VMEM(shape, dtype) for shape, dtype in scratch]
        + [dma((19,)), dma((2,)), dma((2,)), dma((N_OUT,)), dma((N_OUT,))]
        + [dma((plane,))] * 4
        + [dma((nz,))] * 4
        + [regular] * 3,
        compiler_params=pltpu.CompilerParams(
            collective_id=0, has_side_effects=True, vmem_limit_bytes=48 * 1024 * 1024
        ),
        name="layer",
    )(
        *(
            pltpu.with_memory_space_constraint(array, pltpu.HBM)
            for array in (
                hidden,
                query_weight,
                key_weight,
                value_weight,
                head_gate_weight,
                state_in_weight,
                state_gate_weight,
                head_out_weight,
                state_out_weight,
                sink_logit,
                log_step,
                decay_real,
                decay_frequency,
                input_real.transpose(0, 2, 1),
                input_imaginary.transpose(0, 2, 1),
                output_real,
                output_imaginary,
                skip_weight.T,
                decay_shift,
            )
        )
    )


def solution(mesh):
    sizes = SP_SIZES[mesh.shape["sp"]]
    in_specs = (
        P("sp", "tp"),
        P(None, "tp"),
        P(None, "tp"),
        P(None, "tp"),
        P(None, "tp"),
        P(None, "tp"),
        P(None, "tp"),
        P("tp"),
        P("tp", None),
        P("tp", None),
        P("tp"),
        P("tp", None, None),
        P("tp", None, None),
        P("tp", None, None),
        P("tp", None, None),
        P("tp", None),
        P("tp", "sp"),
        P("tp", None),
        P("tp", None),
    )
    return jax.shard_map(
        functools.partial(on_device, sizes),
        mesh=mesh,
        in_specs=in_specs,
        out_specs=P("sp", "tp"),
        check_vma=False,
    )
```
